32 devices in a mesh: ep: 8 (over z, x), tp: 4 (over y, core).
Axes of the slice: x: 2, y: 2, z: 4, core: 2. Of those that a mesh axis runs over, the one named last changes fastest.
Arguments:
- query_latent: bfloat16 [2048, 512], P(('ep', 'tp')), may hold values from -6 to 6
- key_latent: bfloat16 [2048, 256], P(('ep', 'tp')), may hold values from -6 to 6
- rotary_key: bfloat16 [2048, 32], P(('ep', 'tp')), may hold values from -140 to 140
- query_gain: float32 [512], replicated, may hold values from 0.1 to 1.9
- latent_gain: float32 [256], replicated, may hold values from 0.1 to 1.9
- query_content: bfloat16 [512, 512], replicated, may hold values from -0.625 to 0.625
- query_rotary: bfloat16 [512, 256], replicated, may hold values from -0.625 to 0.625
- key_content: bfloat16 [256, 512], replicated, may hold values from -0.375 to 0.375
- value_weight: bfloat16 [256, 512], replicated, may hold values from -0.375 to 0.375
- output_weight: bfloat16 [512, 2048], P('tp'), may hold values from -1 to 1
- expert_input: bfloat16 [2048, 2048], P(('ep', 'tp')), may hold values from -6 to 6
- norm_gain: float32 [2048], replicated, may hold values from 0.1 to 1.9
- routes: int32 [2048, 2], P(('ep', 'tp')), may hold values from 0 to 15, all different within a row; in each aligned block of 64 rows (0 to 63, 64 to 127, ...) at most 16 rows name the same one
- route_weight: float32 [2048, 2], P(('ep', 'tp')), may hold values from 0.25 to 2
- expert_gate: bfloat16 [16, 2048, 1024], P('ep', None, 'tp'), may hold values from -0.125 to 0.125
- expert_up: bfloat16 [16, 2048, 1024], P('ep', None, 'tp'), may hold values from -0.125 to 0.125
- expert_down: bfloat16 [16, 1024, 2048], P('ep', 'tp'), may hold values from -0.1875 to 0.1875
- shared_gate: bfloat16 [2048, 1024], P(None, 'tp'), may hold values from -0.125 to 0.125
- shared_up: bfloat16 [2048, 1024], P(None, 'tp'), may hold values from -0.125 to 0.125
- shared_down: bfloat16 [1024, 2048], P('tp'), may hold values from -0.1875 to 0.1875
Outputs:
- mixer_out: bfloat16 [2048, 2048], P(('ep', 'tp'))
- expert_out: bfloat16 [2048, 2048], P(('ep', 'tp'))
The draws below stay inside these ranges and needn't reach their ends.
Inputs may be any that keep to these rules, and one draw needn't show every extreme that they name: `routes`: each row names 2 different experts. Within the rows of one device (aligned blocks of 64 rows) no expert is named by more than 16 rows, and in every draw some expert is named by exactly 16 rows of some device.
All inputs are finite; a program needn't handle non-finite values.
Results may differ from the reference program's by a relative error of at most 0.013.
The reference program's roundings to bfloat16 on the way count: a program that leaves them out, or rounds other values in their place, can miss the bound.
Values may be sent and summed in bfloat16 or wider, within the bound.
A program may use at most 128 MiB of HBM per device.

```python
import math
from functools import partial
import jax
import jax.numpy as jnp
import numpy as np
from jax import lax

D = 2048
HEADS = 8
CONTENT = 64
ROTARY = 32
VALUE = 64
QUERY_RANK = 512
KEY_RANK = 256
EXPERT_WIDTH = 1024
SHARED_WIDTH = 1024
TOPK = 2
TOK_B = 64
EXPERTS = 16
CAPACITY = 16
TOKENS_A = 2048
TOKENS_B = 2048
N_EP = 8
N_TP = 4


def draw_rotary_key(key, part):
    normal_part = jnp.clip(jax.random.normal(jax.random.fold_in(key, 11), (TOKENS_A, ROTARY), jnp.float32), -6.0, 6.0)
    entries = normal_part
    return entries.astype(jnp.bfloat16)


def block_levels(rng, dims, shards, smallest, top_value):
    level = 1.0
    for dim, blocks in shards:
        draws = jax.random.uniform(jax.random.fold_in(jax.random.fold_in(rng, 6), dim), (blocks,), jnp.float32, smallest / len(shards), top_value / len(shards))
        level = level * jnp.repeat(jnp.exp(draws), dims[dim] // blocks).reshape((-1,) + (1,) * (len(dims) - 1 - dim))
    return level


def deal_out(rng, own, number, rows, amount, top, limit, slope):
    sequence = jax.random.permutation(rng, amount)
    crowded, ordinary = load_shares(amount, rows * top, limit, slope, True), load_shares(amount, rows * top, limit, slope, False)
    places = jnp.arange(amount)

    def named(sizes, turn):
        used = int((sizes > 0).sum())
        fixed = max(1, used // 4)
        moved = fixed + (places - fixed + turn * (used - fixed)) % max(1, amount - fixed)
        return jnp.zeros((amount,), jnp.int32).at[sequence[jnp.where(places < fixed, places, moved)]].set(jnp.asarray(sizes, jnp.int32))

    sizes = jnp.where(number % 4 == 0, named(crowded, number // 4), named(ordinary, number - number // 4 - 1))
    mixed = jax.random.permutation(jax.random.fold_in(own, 3), amount)
    source_of, taker = mixed[0:amount // 2 * 2:2], mixed[1:amount // 2 * 2:2]
    slack = jnp.minimum(sizes[source_of] - 1, limit - sizes[taker]) // 2
    slack = jnp.where((source_of == sequence[0]) | (taker == sequence[0]) | (sizes[taker] == 0), 0, jnp.maximum(slack, 0))
    moved = jax.random.randint(jax.random.fold_in(own, 4), (amount // 2,), 0, 1 << 20) % (slack + 1)
    sizes = sizes.at[source_of].add(-moved).at[taker].add(moved)
    labels = jnp.searchsorted(jnp.cumsum(sizes), jnp.arange(rows * top), side="right").astype(jnp.int32)
    grid = labels.reshape(top, rows).T
    grid = grid[jax.random.permutation(jax.random.fold_in(own, 1), rows)]
    turn = jax.random.randint(jax.random.fold_in(own, 2), (rows, 1), 0, top)
    return jnp.take_along_axis(grid, (jnp.arange(top)[None, :] + turn) % top, axis=1)


def load_shares(number_of, total, limit, skew, full):
    portions = [(1 << 20) // math.isqrt(rank ** skew) + 1 for rank in range(1, number_of + 1)]
    largest = limit if full else min(limit, max(-(-total // number_of), total * portions[0] // sum(portions)))
    least = 1 if total - largest >= number_of - 1 else 0
    holding, surplus = [largest] + [least] * (number_of - 1), total - largest - least * (number_of - 1)
    while surplus > 0:
        movable = [i for i in range(1, number_of) if holding[i] < largest] or [i for i in range(1, number_of) if holding[i] < limit]
        mass, budget = sum([portions[i] for i in movable]), surplus
        for i in movable:
            addition = min(limit - holding[i], max(1, budget * portions[i] // mass), surplus)
            holding[i] = holding[i] + addition
            surplus = surplus - addition
    return np.array(holding)


def gaussian(own_key, dims, scale, reach, pieces=(), held_as=jnp.bfloat16):
    values = jax.random.normal(own_key, dims, jnp.float32) * scale
    if len(pieces) > 0:
        values = block_levels(own_key, dims, pieces, -0.22, 0.18) * values
    return jnp.clip(values, min=-reach, max=reach).astype(held_as)


def setup_inputs(seed: int = 0) -> dict:
    streams_of = jax.random.split(jax.random.key(seed), 21)
    query_latent = gaussian(streams_of[0], (TOKENS_A, QUERY_RANK), 1.0, 6.0, ((0, 32),))
    key_latent = gaussian(streams_of[1], (TOKENS_A, KEY_RANK), 1.0, 6.0, ((0, 32),))
    rotary_key = draw_rotary_key(jax.random.fold_in(streams_of[20], 71), 0)
    query_gain = jnp.clip(1.0 + 0.18 * jax.random.normal(streams_of[3], (QUERY_RANK,), jnp.float32), 0.1, 1.9)
    latent_gain = jnp.clip(1.0 + 0.18 * jax.random.normal(streams_of[4], (KEY_RANK,), jnp.float32), 0.1, 1.9)
    query_content = gaussian(streams_of[5], (QUERY_RANK, HEADS * CONTENT), (QUERY_RANK // 6) ** -0.5, 0.625)
    query_rotary = gaussian(streams_of[6], (QUERY_RANK, HEADS * ROTARY), (QUERY_RANK // 6) ** -0.5, 0.625)
    key_content = gaussian(streams_of[7], (KEY_RANK, HEADS * CONTENT), KEY_RANK ** -0.5, 0.375)
    value_weight = gaussian(streams_of[8], (KEY_RANK, HEADS * VALUE), KEY_RANK ** -0.5, 0.375)
    output_weight = gaussian(streams_of[9], (HEADS * VALUE, D), (HEADS * VALUE // 16) ** -0.5, 1.0, ((0, 4),))
    expert_input = gaussian(streams_of[10], (TOKENS_B, D), 1.0, 6.0, ((0, 32),))
    norm_gain = jnp.clip(1.0 + 0.18 * jax.random.normal(streams_of[11], (D,), jnp.float32), 0.1, 1.9)
    routes_keys = jax.random.split(jax.random.fold_in(streams_of[12], 1), TOKENS_B // TOK_B)
    routes_turns = jax.random.permutation(jax.random.fold_in(streams_of[12], 3), TOKENS_B // TOK_B)
    routes = jax.vmap(lambda own, number: deal_out(jax.random.fold_in(streams_of[12], 2), own, number, TOK_B, EXPERTS, TOPK, CAPACITY, 1))(routes_keys, routes_turns).reshape((TOKENS_B, TOPK))
    route_weight = jnp.clip(0.25 + 1.75 * jax.random.uniform(streams_of[13], (TOKENS_B, TOPK), jnp.float32) ** block_levels(streams_of[13], (TOKENS_B, TOPK), ((0, 32),), -0.2, 0.2), 0.25, 2.0)
    expert_gate = gaussian(streams_of[14], (EXPERTS, D, EXPERT_WIDTH), D ** -0.5, 0.125, ((0, 8), (2, 4)))
    expert_up = gaussian(streams_of[15], (EXPERTS, D, EXPERT_WIDTH), D ** -0.5, 0.125, ((0, 8), (2, 4)))
    expert_down = gaussian(streams_of[16], (EXPERTS, EXPERT_WIDTH, D), EXPERT_WIDTH ** -0.5, 0.1875, ((0, 8), (1, 4)))
    shared_gate = gaussian(streams_of[17], (D, SHARED_WIDTH), D ** -0.5, 0.125, ((1, 4),))
    shared_up = gaussian(streams_of[18], (D, SHARED_WIDTH), D ** -0.5, 0.125, ((1, 4),))
    shared_down = gaussian(streams_of[19], (SHARED_WIDTH, D), SHARED_WIDTH ** -0.5, 0.1875, ((0, 4),))
    return {"query_latent": query_latent, "key_latent": key_latent, "rotary_key": rotary_key, "query_gain": query_gain, "latent_gain": latent_gain, "query_content": query_content, "query_rotary": query_rotary, "key_content": key_content, "value_weight": value_weight, "output_weight": output_weight, "expert_input": expert_input, "norm_gain": norm_gain, "routes": routes, "route_weight": route_weight, "expert_gate": expert_gate, "expert_up": expert_up, "expert_down": expert_down, "shared_gate": shared_gate, "shared_up": shared_up, "shared_down": shared_down}


norm_eps = 1e-06
rope_base = 10000.0

def rms_rows(entries, gain_row):
    widened = entries.astype(jnp.float32)
    return widened * lax.rsqrt(lax.optimization_barrier(jnp.mean(widened * widened, -1, keepdims=True)) + norm_eps) * gain_row.astype(jnp.float32)

def turn_pairs(entries, positions):
    width_full = entries.shape[-1]
    frequency = rope_base ** (-jnp.arange(width_full // 2, dtype=jnp.float32) * 2.0 / width_full)
    angles = positions.astype(jnp.float32)[:, None] * frequency[None, :]
    cosine = jnp.cos(angles)[:, None, :]
    sine_part = jnp.sin(angles)[:, None, :]
    even_part = entries[..., 0::2]
    odd_part = entries[..., 1::2]
    joined = jnp.stack([even_part * cosine - odd_part * sine_part, even_part * sine_part + odd_part * cosine], -1)
    return joined.reshape(entries.shape)

def feed_forward(row_block, gate_weight, up_weight, down_weight, groups):
    gated = jnp.dot(row_block, gate_weight, preferred_element_type=jnp.float32)
    lifted = jnp.dot(row_block, up_weight, preferred_element_type=jnp.float32)
    hidden = (jax.nn.silu(gated) * lifted).astype(jnp.bfloat16)
    group_width = hidden.shape[1] // groups
    running = jnp.zeros((row_block.shape[0], down_weight.shape[1]), jnp.float32)
    for group_index in range(groups):
        product = jnp.dot(hidden[:, group_index * group_width:(group_index + 1) * group_width], down_weight[group_index * group_width:(group_index + 1) * group_width], preferred_element_type=jnp.float32)
        running = running + lax.optimization_barrier(product.astype(jnp.bfloat16)).astype(jnp.float32)
    return running

def attend_queries(query_blocks, key_wide, turn_wide, value_wide):
    query_part, query_turn = query_blocks
    score_scale = (CONTENT + ROTARY) ** (-0.5)
    scores = jnp.einsum('qhc,khc->qhk', query_part.astype(jnp.float32), key_wide)
    scores = scores + jnp.einsum('qhr,kr->qhk', query_turn.astype(jnp.float32), turn_wide)
    scores = scores * score_scale
    weights = jnp.exp(scores - lax.optimization_barrier(jnp.max(scores, -1, keepdims=True)))
    denominator = lax.optimization_barrier(jnp.sum(weights, -1))
    rounded = lax.optimization_barrier(weights.astype(jnp.bfloat16)).astype(jnp.float32)
    numerator = jnp.einsum('qhk,khv->qhv', rounded, value_wide)
    return (numerator / denominator[..., None]).astype(jnp.bfloat16)

def block_slots(route_block):
    flat_routes = route_block.reshape(-1)
    marks = (flat_routes[:, None] == jnp.arange(EXPERTS, dtype=jnp.int32)[None, :]).astype(jnp.int32)
    return lax.optimization_barrier(jnp.sum((jnp.cumsum(marks, 0) - marks) * marks, 1)).reshape(route_block.shape)

def reference(query_latent, key_latent, rotary_key, query_gain, latent_gain, query_content, query_rotary, key_content, value_weight, output_weight, expert_input, norm_gain, routes, route_weight, expert_gate, expert_up, expert_down, shared_gate, shared_up, shared_down):
    row_count = query_latent.shape[0]
    positions = jnp.arange(row_count, dtype=jnp.int32)
    query_normed = rms_rows(query_latent, query_gain).astype(jnp.bfloat16)
    latent_normed = rms_rows(key_latent, latent_gain).astype(jnp.bfloat16)
    query_part = jnp.dot(query_normed, query_content, preferred_element_type=jnp.float32).astype(jnp.bfloat16).reshape(row_count, HEADS, CONTENT)
    query_turn = turn_pairs(jnp.dot(query_normed, query_rotary, preferred_element_type=jnp.float32).reshape(row_count, HEADS, ROTARY), positions).astype(jnp.bfloat16)
    key_turn = turn_pairs(rotary_key.astype(jnp.float32)[:, None, :], positions)[:, 0, :].astype(jnp.bfloat16)
    key_part = jnp.dot(latent_normed, key_content, preferred_element_type=jnp.float32).astype(jnp.bfloat16).reshape(row_count, HEADS, CONTENT)
    value_rows = jnp.dot(latent_normed, value_weight, preferred_element_type=jnp.float32).astype(jnp.bfloat16).reshape(row_count, HEADS, VALUE)
    query_block = math.gcd(row_count, 256)
    block_count = row_count // query_block
    query_blocks = (query_part.reshape(block_count, query_block, HEADS, CONTENT), query_turn.reshape(block_count, query_block, HEADS, ROTARY))
    attended = lax.map(partial(attend_queries, key_wide=key_part.astype(jnp.float32), turn_wide=key_turn.astype(jnp.float32), value_wide=value_rows.astype(jnp.float32)), query_blocks)
    attended = attended.reshape(row_count, HEADS * VALUE)
    group_width = HEADS * VALUE // N_TP
    mixed = jnp.zeros((row_count, output_weight.shape[1]), jnp.float32)
    for group_index in range(N_TP):
        product = jnp.dot(attended[:, group_index * group_width:(group_index + 1) * group_width], output_weight[group_index * group_width:(group_index + 1) * group_width], preferred_element_type=jnp.float32)
        mixed = mixed + lax.optimization_barrier(product.astype(jnp.bfloat16)).astype(jnp.float32)
    mixer_out = mixed.astype(jnp.bfloat16)
    token_count = expert_input.shape[0]
    device_count = N_EP * N_TP
    per_device = token_count // device_count
    expert_normed = rms_rows(expert_input, norm_gain).astype(jnp.bfloat16)
    slots = jax.vmap(block_slots)(routes.reshape(device_count, per_device, TOPK)).reshape(token_count, TOPK)
    device_of = (jnp.arange(token_count, dtype=jnp.int32) // per_device).astype(jnp.int32)
    token_index = jnp.broadcast_to(jnp.arange(token_count, dtype=jnp.int32)[:, None], (token_count, TOPK))
    table = jnp.full((EXPERTS, device_count, CAPACITY), token_count, jnp.int32)
    table = table.at[routes, jnp.broadcast_to(device_of[:, None], (token_count, TOPK)), slots].set(token_index)
    padded = jnp.concatenate([expert_normed, jnp.zeros((1, expert_normed.shape[1]), jnp.bfloat16)], 0)

    def one_expert(expert_args):
        table_row, gate_weight, up_weight, down_weight = expert_args
        row_block = padded[table_row.reshape(-1)]
        return feed_forward(row_block, gate_weight, up_weight, down_weight, N_TP).astype(jnp.bfloat16)
    results = lax.map(one_expert, (table, expert_gate, expert_up, expert_down))
    flat_index = (routes * (device_count * CAPACITY) + device_of[:, None] * CAPACITY + slots).astype(jnp.int32)
    picked = results.reshape(-1, results.shape[-1])[flat_index.reshape(-1)].reshape(token_count, TOPK, -1)
    routed = lax.optimization_barrier(jnp.sum(route_weight.astype(jnp.float32)[..., None] * picked.astype(jnp.float32), 1))
    shared_sum = feed_forward(expert_normed, shared_gate, shared_up, shared_down, N_TP)
    expert_out = (routed + shared_sum).astype(jnp.bfloat16)
    return (mixer_out, expert_out)
```

```python
import math

import jax
import jax.numpy as jnp
from jax import lax
from jax.experimental import pallas as pl
from jax.experimental.pallas import tpu as pltpu
from jax.sharding import PartitionSpec as P

HEADS = 8
CONTENT = 64
ROTARY = 32
VALUE = 64


norm_eps = 1e-06
rope_base = 10000.0


def rms_rows(entries, gain_row):
    widened = entries.astype(jnp.float32)
    return widened * lax.rsqrt(jnp.mean(widened * widened, -1, keepdims=True) + norm_eps) * gain_row


def turn_pairs(entries, positions):
    width_full = entries.shape[-1]
    frequency = rope_base ** (-jnp.arange(width_full // 2, dtype=jnp.float32) * 2.0 / width_full)
    angles = positions.astype(jnp.float32)[:, None] * frequency[None, :]
    cosine = jnp.cos(angles)[:, None, :]
    sine_part = jnp.sin(angles)[:, None, :]
    even_part = entries[..., 0::2]
    odd_part = entries[..., 1::2]
    joined = jnp.stack(
        [even_part * cosine - odd_part * sine_part, even_part * sine_part + odd_part * cosine], -1
    )
    return joined.reshape(entries.shape)


def absorb_block(carried, query_part, query_turn, key_part, key_turn, value_rows, score_scale):
    running_peak, running_total, summed = carried
    scores = jnp.einsum("qhc,khc->qhk", query_part, key_part, preferred_element_type=jnp.float32)
    scores = scores + jnp.einsum(
        "qhr,kr->qhk", query_turn, key_turn, preferred_element_type=jnp.float32
    )
    scores = scores * score_scale
    new_peak = jnp.maximum(running_peak, jnp.max(scores, -1))
    factor = jnp.exp(running_peak - new_peak)
    weights = jnp.exp(scores - new_peak[..., None])
    running_total = running_total * factor + jnp.sum(weights, -1)
    summed = summed * factor[..., None] + jnp.einsum(
        "qhk,khv->qhv", weights.astype(jnp.bfloat16), value_rows, preferred_element_type=jnp.float32
    )
    return (new_peak, running_total, summed)


def absorb_piece(carried, query_part, query_turn, key_part, key_turn, value_rows, score_scale):
    row_count = key_part.shape[0]
    key_block = math.gcd(row_count, 2048)
    if key_block == row_count:
        return absorb_block(
            carried, query_part, query_turn, key_part, key_turn, value_rows, score_scale
        )
    block_count = row_count // key_block

    def advance(state, pieces):
        return (
            absorb_block(
                state, query_part, query_turn, pieces[0], pieces[1], pieces[2], score_scale
            ),
            None,
        )

    stacked = (
        key_part.reshape((block_count, key_block) + key_part.shape[1:]),
        key_turn.reshape(block_count, key_block, key_turn.shape[1]),
        value_rows.reshape((block_count, key_block) + value_rows.shape[1:]),
    )
    carried, ignored = lax.scan(advance, carried, stacked)
    return carried


def expand_keys(latent_rows, key_columns, value_columns, head_local):
    row_count = latent_rows.shape[0]
    key_part = (
        jnp.dot(latent_rows, key_columns, preferred_element_type=jnp.float32)
        .astype(jnp.bfloat16)
        .reshape(row_count, head_local, CONTENT)
    )
    value_rows = (
        jnp.dot(latent_rows, value_columns, preferred_element_type=jnp.float32)
        .astype(jnp.bfloat16)
        .reshape(row_count, head_local, VALUE)
    )
    return (key_part, value_rows)


def expert_terms(row_block, gate_weight, up_weight, down_weight):
    gated = jnp.einsum("secd,edf->secf", row_block, gate_weight, preferred_element_type=jnp.float32)
    lifted = jnp.einsum("secd,edf->secf", row_block, up_weight, preferred_element_type=jnp.float32)
    hidden = (jax.nn.silu(gated) * lifted).astype(jnp.bfloat16)
    return jnp.einsum("secf,efd->secd", hidden, down_weight, preferred_element_type=jnp.float32)


def shared_terms(row_block, gate_weight, up_weight, down_weight):
    gated = jnp.dot(row_block, gate_weight, preferred_element_type=jnp.float32)
    lifted = jnp.dot(row_block, up_weight, preferred_element_type=jnp.float32)
    hidden = (jax.nn.silu(gated) * lifted).astype(jnp.bfloat16)
    return jnp.dot(hidden, down_weight, preferred_element_type=jnp.float32)


def shards_plain(
    query_latent,
    key_latent,
    rotary_key,
    query_gain,
    latent_gain,
    query_content,
    query_rotary,
    key_content,
    value_weight,
    output_weight,
    expert_input,
    norm_gain,
    routes,
    route_weight,
    expert_gate,
    expert_up,
    expert_down,
    shared_gate,
    shared_up,
    shared_down,
):
    group_size = lax.axis_size("tp")
    expert_groups = lax.axis_size("ep")
    own_rows = query_latent.shape[0]
    head_local = HEADS // group_size
    head_index = lax.axis_index("tp")
    group_rows_count = own_rows * group_size
    group_start = lax.axis_index("ep") * group_rows_count
    own_start = group_start + head_index * own_rows
    score_scale = (CONTENT + ROTARY) ** (-0.5)
    query_normed = rms_rows(query_latent, query_gain).astype(jnp.bfloat16)
    latent_normed = rms_rows(key_latent, latent_gain).astype(jnp.bfloat16)
    own_positions = own_start + jnp.arange(own_rows, dtype=jnp.int32)
    key_turned = turn_pairs(rotary_key.astype(jnp.float32)[:, None, :], own_positions)[
        :, 0, :
    ].astype(jnp.bfloat16)
    token_rows = expert_input.shape[0]
    picks = routes.shape[1]
    local_experts = expert_gate.shape[0]
    expert_total = local_experts * expert_groups
    capacity = 2 * token_rows * picks // expert_total
    slot_total = expert_total * capacity
    model_width = expert_input.shape[1]
    expert_normed = rms_rows(expert_input, norm_gain).astype(jnp.bfloat16)
    flat_routes = routes.reshape(-1)
    marks = (flat_routes[:, None] == jnp.arange(expert_total, dtype=jnp.int32)[None, :]).astype(
        jnp.int32
    )
    ranks = jnp.sum((jnp.cumsum(marks, 0) - marks) * marks, 1)
    targets = flat_routes * capacity + ranks
    picker = (jnp.arange(slot_total, dtype=jnp.int32)[:, None] == targets[None, :]).astype(
        jnp.int32
    )
    picker = jnp.sum(picker.reshape(slot_total, token_rows, picks), 2).astype(jnp.bfloat16)
    outgoing = jnp.dot(picker, expert_normed, preferred_element_type=jnp.float32).astype(
        jnp.bfloat16
    )
    outgoing = outgoing.reshape(expert_groups, local_experts, capacity, model_width)
    received = lax.all_to_all(outgoing, "ep", split_axis=0, concat_axis=0, tiled=True)
    group_query, group_latent, group_turn, gathered_rows, gathered_tokens = (
        lax.all_gather(query_normed, "tp", axis=0, tiled=True),
        lax.all_gather(latent_normed, "tp", axis=0, tiled=True),
        lax.all_gather(key_turned, "tp", axis=0, tiled=True),
        lax.all_gather(received, "tp", axis=0, tiled=True),
        lax.all_gather(expert_normed, "tp", axis=0, tiled=True),
    )
    positions = group_start + jnp.arange(group_rows_count, dtype=jnp.int32)
    content_columns = lax.dynamic_slice_in_dim(
        query_content, head_index * head_local * CONTENT, head_local * CONTENT, 1
    )
    rotary_columns = lax.dynamic_slice_in_dim(
        query_rotary, head_index * head_local * ROTARY, head_local * ROTARY, 1
    )
    query_part = (
        jnp.dot(group_query, content_columns, preferred_element_type=jnp.float32)
        .astype(jnp.bfloat16)
        .reshape(group_rows_count, head_local, CONTENT)
    )
    query_turn = turn_pairs(
        jnp.dot(group_query, rotary_columns, preferred_element_type=jnp.float32).reshape(
            group_rows_count, head_local, ROTARY
        ),
        positions,
    ).astype(jnp.bfloat16)
    key_columns = lax.dynamic_slice_in_dim(
        key_content, head_index * head_local * CONTENT, head_local * CONTENT, 1
    )
    value_columns = lax.dynamic_slice_in_dim(
        value_weight, head_index * head_local * VALUE, head_local * VALUE, 1
    )
    carry_start = (
        jnp.full((group_rows_count, head_local), -jnp.inf, jnp.float32),
        jnp.zeros((group_rows_count, head_local), jnp.float32),
        jnp.zeros((group_rows_count, head_local, VALUE), jnp.float32),
    )
    key_part, value_rows = expand_keys(
        lax.all_gather(group_latent, "ep", axis=0, tiled=True),
        key_columns,
        value_columns,
        head_local,
    )
    running_peak, running_total, summed = absorb_piece(
        carry_start,
        query_part,
        query_turn,
        key_part,
        lax.all_gather(group_turn, "ep", axis=0, tiled=True),
        value_rows,
        score_scale,
    )
    attended = (
        (summed / running_total[..., None])
        .astype(jnp.bfloat16)
        .reshape(group_rows_count, head_local * VALUE)
    )
    routed_term = expert_terms(gathered_rows, expert_gate, expert_up, expert_down)
    shared_term = shared_terms(gathered_tokens, shared_gate, shared_up, shared_down)
    mixer_term = jnp.dot(attended, output_weight, preferred_element_type=jnp.float32)
    mixer_sum, routed_sum, shared_sum = (
        lax.psum_scatter(
            mixer_term.astype(jnp.bfloat16), "tp", scatter_dimension=0, tiled=True
        ).astype(jnp.float32),
        lax.psum_scatter(
            routed_term.astype(jnp.bfloat16), "tp", scatter_dimension=0, tiled=True
        ).astype(jnp.float32),
        lax.psum_scatter(
            shared_term.astype(jnp.bfloat16), "tp", scatter_dimension=0, tiled=True
        ).astype(jnp.float32),
    )
    mixer_out = mixer_sum.astype(jnp.bfloat16)
    returned = lax.all_to_all(
        routed_sum.astype(jnp.bfloat16), "ep", split_axis=0, concat_axis=0, tiled=True
    )
    returned = returned.reshape(slot_total, model_width)
    picked = jnp.take(returned, targets, axis=0).reshape(token_rows, picks, model_width)
    combined = jnp.sum(route_weight[..., None] * picked.astype(jnp.float32), 1) + shared_sum
    expert_out = combined.astype(jnp.bfloat16)
    return (mixer_out, expert_out)


MESH = pl.DeviceIdType.MESH
VMEM_LIMIT = 60 * 1024 * 1024


def greet(ep_count, me, head_index):
    barrier = pltpu.get_barrier_semaphore()
    for step in range(1, ep_count):
        pl.semaphore_signal(
            barrier, inc=1, device_id=(lax.rem(me + step, ep_count), head_index), device_id_type=MESH
        )
    row, core = head_index // 2, head_index % 2
    for other in ((1 - row) * 2 + core, row * 2 + 1 - core):
        pl.semaphore_signal(barrier, inc=1, device_id=(me, other), device_id_type=MESH)
    pl.semaphore_wait(barrier, ep_count + 1)


def spread_kernel(
    ep_count,
    slots_ref,
    latent_ref,
    tokens_ref,
    query_ref,
    rows_out,
    latent_out,
    tokens_out,
    query_out,
    ep_send,
    ep_recv,
    y_send,
    y_recv,
    core_send,
    core_recv,
    cross_send,
    cross_recv,
    own_sem,
):
    me = lax.axis_index("ep")
    head_index = lax.axis_index("tp")
    row, core = head_index // 2, head_index % 2
    y_peer = (me, (1 - row) * 2 + core)
    core_peer = (me, row * 2 + 1 - core)
    greet(ep_count, me, head_index)

    def remote(source, target, send_sem, recv_sem, device):
        return pltpu.make_async_remote_copy(
            src_ref=source,
            dst_ref=target,
            send_sem=send_sem,
            recv_sem=recv_sem,
            device_id=device,
            device_id_type=MESH,
        )

    def ep_copies(step):
        peer = lax.rem(me + step, ep_count)
        return (
            remote(
                latent_ref,
                latent_out.at[row, core, me],
                ep_send.at[1, step],
                ep_recv.at[1, step],
                (peer, head_index),
            ),
            remote(
                slots_ref.at[peer],
                rows_out.at[row, core, me],
                ep_send.at[0, step],
                ep_recv.at[0, step],
                (peer, head_index),
            ),
        )

    def block_copies(origin_row, step, send_sem, recv_sem, device):
        origin = lax.rem(me + ep_count - step, ep_count)
        return (
            remote(
                latent_out.at[origin_row, core, origin],
                latent_out.at[origin_row, core, origin],
                send_sem.at[1, step],
                recv_sem.at[1, step],
                device,
            ),
            remote(
                rows_out.at[origin_row, core, origin],
                rows_out.at[origin_row, core, origin],
                send_sem.at[0, step],
                recv_sem.at[0, step],
                device,
            ),
        )

    def group_copies(origin_row, send_sem, recv_sem, device):
        return (
            remote(
                tokens_out.at[origin_row, core],
                tokens_out.at[origin_row, core],
                send_sem.at[0, ep_count],
                recv_sem.at[0, ep_count],
                device,
            ),
            remote(
                query_out.at[origin_row, core],
                query_out.at[origin_row, core],
                send_sem.at[1, ep_count],
                recv_sem.at[1, ep_count],
                device,
            ),
        )

    own = (
        pltpu.make_async_copy(latent_ref, latent_out.at[row, core, me], own_sem.at[0]),
        pltpu.make_async_copy(slots_ref.at[me], rows_out.at[row, core, me], own_sem.at[1]),
        pltpu.make_async_copy(tokens_ref, tokens_out.at[row, core], own_sem.at[2]),
        pltpu.make_async_copy(query_ref, query_out.at[row, core], own_sem.at[3]),
    )
    for copy in own:
        copy.start()
    for step in range(1, ep_count):
        for copy in ep_copies(step):
            copy.start()
    for copy in own:
        copy.wait()
    own_row, far_row = row, 1 - row
    for copy in group_copies(own_row, y_send, y_recv, y_peer):
        copy.start()
    for copy in group_copies(own_row, core_send, core_recv, core_peer):
        copy.start()
    for step in range(ep_count + 1):
        if step < ep_count:
            if step > 0:
                for copy in ep_copies(step):
                    copy.wait_recv()
            for copy in block_copies(own_row, step, y_send, y_recv, y_peer):
                copy.start()
            for copy in block_copies(own_row, step, core_send, core_recv, core_peer):
                copy.start()
        if step == 0:
            for copy in group_copies(own_row, y_send, y_recv, y_peer):
                copy.wait_recv()
            for copy in group_copies(far_row, cross_send, cross_recv, core_peer):
                copy.start()
        else:
            for copy in block_copies(own_row, step - 1, y_send, y_recv, y_peer):
                copy.wait_recv()
            for copy in block_copies(far_row, step - 1, cross_send, cross_recv, core_peer):
                copy.start()
    for step in range(1, ep_count):
        for copy in ep_copies(step):
            copy.wait_send()
    waits = [
        (own_row, y_send, y_recv, y_peer, False),
        (own_row, core_send, core_recv, core_peer, True),
        (far_row, cross_send, cross_recv, core_peer, True),
    ]
    for origin_row, send_sem, recv_sem, device, both in waits:
        for copy in group_copies(origin_row, send_sem, recv_sem, device):
            copy.wait_send()
            if both:
                copy.wait_recv()
        for step in range(ep_count):
            for copy in block_copies(origin_row, step, send_sem, recv_sem, device):
                copy.wait_send()
                if both:
                    copy.wait_recv()


def spread(slots, latent_pack, tokens, queries):
    ep_count, row_count, width = slots.shape
    vmem = pl.BlockSpec(memory_space=pltpu.VMEM)
    semaphores = pltpu.SemaphoreType.DMA((2, ep_count + 1))
    return pl.pallas_call(
        lambda *refs: spread_kernel(ep_count, *refs),
        out_shape=(
            jax.ShapeDtypeStruct((2, 2, ep_count, row_count, width), jnp.bfloat16),
            jax.ShapeDtypeStruct((2, 2, ep_count) + latent_pack.shape, jnp.bfloat16),
            jax.ShapeDtypeStruct((2, 2) + tokens.shape, jnp.bfloat16),
            jax.ShapeDtypeStruct((2, 2) + queries.shape, jnp.bfloat16),
        ),
        in_specs=[vmem] * 4,
        out_specs=(vmem,) * 4,
        scratch_shapes=[semaphores] * 8 + [pltpu.SemaphoreType.DMA((4,))],
        compiler_params=pltpu.CompilerParams(
            collective_id=0, has_side_effects=True, vmem_limit_bytes=VMEM_LIMIT
        ),
        name="spread",
    )(slots, latent_pack, tokens, queries)


def gated_rows(rows, gate_weight, up_weight):
    gated = jnp.dot(rows, gate_weight, preferred_element_type=jnp.float32)
    lifted = jnp.dot(rows, up_weight, preferred_element_type=jnp.float32)
    return (gated / (1.0 + jnp.exp(-gated)) * lifted).astype(jnp.bfloat16)


def finish_kernel(
    ep_count,
    capacity,
    rows_ref,
    tokens_ref,
    mixer_ref,
    gate_ref,
    up_ref,
    down_ref,
    shared_gate_ref,
    shared_up_ref,
    shared_down_ref,
    weight_ref,
    mixer_out,
    expert_out,
    part,
    side,
    half_rows,
    half_side,
    far_rows,
    far_side,
    returned,
    core_send,
    core_recv,
    y_send,
    y_recv,
    ep_send,
    ep_recv,
):
    me = lax.axis_index("ep")
    head_index = lax.axis_index("tp")
    row, core = head_index // 2, head_index % 2
    y_peer = (me, (1 - row) * 2 + core)
    core_peer = (me, row * 2 + 1 - core)
    greet(ep_count, me, head_index)
    local_experts = gate_ref.shape[0]
    width = rows_ref.shape[-1]
    own_rows = tokens_ref.shape[2]
    slot_rows = rows_ref.shape[3]
    stripe = math.gcd(width, 512)

    def remote(source, target, send_sem, recv_sem, device):
        return pltpu.make_async_remote_copy(
            src_ref=source,
            dst_ref=target,
            send_sem=send_sem,
            recv_sem=recv_sem,
            device_id=device,
            device_id_type=MESH,
        )

    def compute(side_core):
        for expert in range(local_experts):
            span = slice(expert * capacity, (expert + 1) * capacity)
            block = rows_ref[:, side_core, :, span, :].reshape(2 * ep_count * capacity, width)
            hidden = gated_rows(block, gate_ref[expert], up_ref[expert])
            for start in range(0, width, stripe):
                product = jnp.dot(
                    hidden,
                    down_ref[expert, :, start : start + stripe],
                    preferred_element_type=jnp.float32,
                ).astype(jnp.bfloat16)
                part[:, side_core, :, span, start : start + stripe] = product.reshape(
                    2, ep_count, capacity, stripe
                )
        block = tokens_ref[:, side_core].reshape(2 * own_rows, width)
        hidden = gated_rows(block, shared_gate_ref[...], shared_up_ref[...])
        for start in range(0, width, stripe):
            product = jnp.dot(
                hidden,
                shared_down_ref[:, start : start + stripe],
                preferred_element_type=jnp.float32,
            ).astype(jnp.bfloat16)
            side[:, side_core, :own_rows, start : start + stripe] = product.reshape(
                2, own_rows, stripe
            )
        side[:, side_core, own_rows:, :] = mixer_ref[:, side_core]

    def core_copies(target_row, place):
        return (
            remote(
                part.at[target_row, 1 - core],
                half_rows.at[target_row],
                core_send.at[place, 0],
                core_recv.at[place, 0],
                core_peer,
            ),
            remote(
                side.at[target_row, 1 - core],
                half_side.at[target_row],
                core_send.at[place, 1],
                core_recv.at[place, 1],
                core_peer,
            ),
        )

    compute(1 - core)
    near, far = core_copies(row, 0), core_copies(1 - row, 1)
    for copy in far + near:
        copy.start()
    compute(core)

    def y_copy(block):
        return remote(
            part.at[1 - row, core, block],
            far_rows.at[block],
            y_send.at[block],
            y_recv.at[block],
            y_peer,
        )

    def ep_copy(step):
        peer = lax.rem(me + step, ep_count)
        return remote(
            part.at[row, core, peer],
            returned.at[me],
            ep_send.at[step],
            ep_recv.at[step],
            (peer, head_index),
        )

    side_copy = remote(
        side.at[1 - row, core], far_side, y_send.at[ep_count], y_recv.at[ep_count], y_peer
    )
    far[0].wait_recv()
    for step in range(ep_count):
        block = lax.rem(me + step + 1, ep_count)
        part[1 - row, core, block] = (
            part[1 - row, core, block].astype(jnp.float32)
            + half_rows[1 - row, block].astype(jnp.float32)
        ).astype(jnp.bfloat16)
        y_copy(block).start()
    far[1].wait_recv()
    side[1 - row, core] = (
        side[1 - row, core].astype(jnp.float32) + half_side[1 - row].astype(jnp.float32)
    ).astype(jnp.bfloat16)
    side_copy.start()
    near[0].wait_recv()
    for step in range(ep_count):
        block = lax.rem(me + step + 1, ep_count)
        y_copy(block).wait_recv()
        total = (
            part[row, core, block].astype(jnp.float32)
            + half_rows[row, block].astype(jnp.float32)
            + far_rows[block].astype(jnp.float32)
        ).astype(jnp.bfloat16)
        if step + 1 < ep_count:
            part[row, core, block] = total
            ep_copy(step + 1).start()
        else:
            returned[me] = total
    near[1].wait_recv()
    side_copy.wait_recv()
    side_total = (
        side[row, core].astype(jnp.float32)
        + half_side[row].astype(jnp.float32)
        + far_side[...].astype(jnp.float32)
    )
    mixer_out[...] = side_total[own_rows:].astype(jnp.bfloat16)
    for step in range(1, ep_count):
        ep_copy(step).wait_recv()
    for start in range(0, width, stripe):
        picked = jnp.dot(
            weight_ref[...],
            returned[:, :, start : start + stripe].reshape(ep_count * slot_rows, stripe),
            preferred_element_type=jnp.float32,
        )
        picked = picked[:own_rows] + picked[own_rows : 2 * own_rows] + picked[2 * own_rows :]
        expert_out[:, start : start + stripe] = (
            picked + side_total[:own_rows, start : start + stripe]
        ).astype(jnp.bfloat16)
    for copy in far + near:
        copy.wait_send()
    for block in range(ep_count):
        y_copy(block).wait_send()
    side_copy.wait_send()
    for step in range(1, ep_count):
        ep_copy(step).wait_send()


def finish(capacity, *operands):
    rows, tokens = operands[0], operands[1]
    ep_count, slot_rows, width = rows.shape[2:]
    own_rows = tokens.shape[2]
    vmem = pl.BlockSpec(memory_space=pltpu.VMEM)
    out = jax.ShapeDtypeStruct((own_rows, width), jnp.bfloat16)
    return pl.pallas_call(
        lambda *refs: finish_kernel(ep_count, capacity, *refs),
        out_shape=(out, out),
        in_specs=[vmem] * len(operands),
        out_specs=(vmem, vmem),
        scratch_shapes=[
            pltpu.VMEM(rows.shape, jnp.bfloat16),
            pltpu.VMEM((2, 2, 2 * own_rows, width), jnp.bfloat16),
            pltpu.VMEM((2, ep_count, slot_rows, width), jnp.bfloat16),
            pltpu.VMEM((2, 2 * own_rows, width), jnp.bfloat16),
            pltpu.VMEM((ep_count, slot_rows, width), jnp.bfloat16),
            pltpu.VMEM((2 * own_rows, width), jnp.bfloat16),
            pltpu.VMEM((ep_count, slot_rows, width), jnp.bfloat16),
            pltpu.SemaphoreType.DMA((2, 2)),
            pltpu.SemaphoreType.DMA((2, 2)),
            pltpu.SemaphoreType.DMA((ep_count + 1,)),
            pltpu.SemaphoreType.DMA((ep_count + 1,)),
            pltpu.SemaphoreType.DMA((ep_count,)),
            pltpu.SemaphoreType.DMA((ep_count,)),
        ],
        compiler_params=pltpu.CompilerParams(
            collective_id=1, has_side_effects=True, vmem_limit_bytes=VMEM_LIMIT
        ),
        name="finish",
    )(*operands)


def shards(
    query_latent,
    key_latent,
    rotary_key,
    query_gain,
    latent_gain,
    query_content,
    query_rotary,
    key_content,
    value_weight,
    output_weight,
    expert_input,
    norm_gain,
    routes,
    route_weight,
    expert_gate,
    expert_up,
    expert_down,
    shared_gate,
    shared_up,
    shared_down,
):
    group_size = lax.axis_size("tp")
    expert_groups = lax.axis_size("ep")
    token_rows = expert_input.shape[0]
    picks = routes.shape[1]
    local_experts = expert_gate.shape[0]
    expert_total = local_experts * expert_groups
    capacity = 2 * token_rows * picks // expert_total
    if group_size != 4 or capacity % 16:
        return shards_plain(
            query_latent,
            key_latent,
            rotary_key,
            query_gain,
            latent_gain,
            query_content,
            query_rotary,
            key_content,
            value_weight,
            output_weight,
            expert_input,
            norm_gain,
            routes,
            route_weight,
            expert_gate,
            expert_up,
            expert_down,
            shared_gate,
            shared_up,
            shared_down,
        )
    own_rows = query_latent.shape[0]
    head_local = HEADS // group_size
    head_index = lax.axis_index("tp")
    group_rows_count = own_rows * group_size
    group_start = lax.axis_index("ep") * group_rows_count
    own_start = group_start + head_index * own_rows
    score_scale = (CONTENT + ROTARY) ** (-0.5)
    query_normed = rms_rows(query_latent, query_gain).astype(jnp.bfloat16)
    latent_normed = rms_rows(key_latent, latent_gain).astype(jnp.bfloat16)
    own_positions = own_start + jnp.arange(own_rows, dtype=jnp.int32)
    key_turned = turn_pairs(rotary_key.astype(jnp.float32)[:, None, :], own_positions)[
        :, 0, :
    ].astype(jnp.bfloat16)
    slot_total = expert_total * capacity
    model_width = expert_input.shape[1]
    expert_normed = rms_rows(expert_input, norm_gain).astype(jnp.bfloat16)
    flat_routes = routes.reshape(-1)
    marks = (flat_routes[:, None] == jnp.arange(expert_total, dtype=jnp.int32)[None, :]).astype(
        jnp.int32
    )
    ranks = jnp.sum((jnp.cumsum(marks, 0) - marks) * marks, 1)
    targets = (flat_routes * capacity + ranks).reshape(token_rows, picks)
    chosen = targets[:, :, None] == jnp.arange(slot_total, dtype=jnp.int32)[None, None, :]
    picker = jnp.any(chosen, 1).astype(jnp.bfloat16)
    spread_weight = jnp.sum(jnp.where(chosen, route_weight[:, :, None], 0.0), 1)
    high = lax.reduce_precision(spread_weight, 8, 7)
    middle = lax.reduce_precision(spread_weight - high, 8, 7)
    low = spread_weight - high - middle
    weight_terms = jnp.concatenate([high, middle, low], 0).astype(jnp.bfloat16)
    slots = lax.dot_general(
        picker, expert_normed, (((0,), (0,)), ((), ())), preferred_element_type=jnp.float32
    ).astype(jnp.bfloat16)
    slots = slots.reshape(expert_groups, local_experts * capacity, model_width)
    rank_width = latent_normed.shape[1]
    pad_width = -rotary_key.shape[1] % 128
    latent_pack = jnp.concatenate(
        [latent_normed, key_turned, jnp.zeros((own_rows, pad_width), jnp.bfloat16)], 1
    )
    gathered_rows, packs, gathered_tokens, group_query = spread(
        slots, latent_pack, expert_normed, query_normed
    )
    packs = (
        packs.reshape(group_size, expert_groups, own_rows, -1)
        .transpose(1, 0, 2, 3)
        .reshape(expert_groups * group_rows_count, -1)
    )
    group_query = group_query.reshape(group_rows_count, -1)
    positions = group_start + jnp.arange(group_rows_count, dtype=jnp.int32)
    content_columns = lax.dynamic_slice_in_dim(
        query_content, head_index * head_local * CONTENT, head_local * CONTENT, 1
    )
    rotary_columns = lax.dynamic_slice_in_dim(
        query_rotary, head_index * head_local * ROTARY, head_local * ROTARY, 1
    )
    query_part = (
        jnp.dot(group_query, content_columns, preferred_element_type=jnp.float32)
        .astype(jnp.bfloat16)
        .reshape(group_rows_count, head_local, CONTENT)
    )
    query_turn = turn_pairs(
        jnp.dot(group_query, rotary_columns, preferred_element_type=jnp.float32).reshape(
            group_rows_count, head_local, ROTARY
        ),
        positions,
    ).astype(jnp.bfloat16)
    key_columns = lax.dynamic_slice_in_dim(
        key_content, head_index * head_local * CONTENT, head_local * CONTENT, 1
    )
    value_columns = lax.dynamic_slice_in_dim(
        value_weight, head_index * head_local * VALUE, head_local * VALUE, 1
    )
    carry_start = (
        jnp.full((group_rows_count, head_local), -jnp.inf, jnp.float32),
        jnp.zeros((group_rows_count, head_local), jnp.float32),
        jnp.zeros((group_rows_count, head_local, VALUE), jnp.float32),
    )
    key_part, value_rows = expand_keys(
        packs[:, :rank_width], key_columns, value_columns, head_local
    )
    running_peak, running_total, summed = absorb_piece(
        carry_start,
        query_part,
        query_turn,
        key_part,
        packs[:, rank_width : rank_width + rotary_key.shape[1]],
        value_rows,
        score_scale,
    )
    attended = (
        (summed / running_total[..., None])
        .astype(jnp.bfloat16)
        .reshape(group_rows_count, head_local * VALUE)
    )
    mixer_term = (
        jnp.dot(attended, output_weight, preferred_element_type=jnp.float32)
        .astype(jnp.bfloat16)
        .reshape(2, 2, own_rows, model_width)
    )
    return finish(
        capacity,
        gathered_rows,
        gathered_tokens,
        mixer_term,
        expert_gate,
        expert_up,
        expert_down,
        shared_gate,
        shared_up,
        shared_down,
        weight_terms,
    )


def solution(mesh):
    in_specs = (
        P(("ep", "tp"), None),
        P(("ep", "tp"), None),
        P(("ep", "tp"), None),
        P(),
        P(),
        P(),
        P(),
        P(),
        P(),
        P("tp", None),
        P(("ep", "tp"), None),
        P(),
        P(("ep", "tp"), None),
        P(("ep", "tp"), None),
        P("ep", None, "tp"),
        P("ep", None, "tp"),
        P("ep", "tp", None),
        P(None, "tp"),
        P(None, "tp"),
        P("tp", None),
    )
    out_specs = (P(("ep", "tp"), None), P(("ep", "tp"), None))
    return jax.shard_map(shards, mesh=mesh, in_specs=in_specs, out_specs=out_specs, check_vma=False)
```

```python
import math

import jax
import jax.numpy as jnp
from jax import lax
from jax.experimental import pallas as pl
from jax.experimental.pallas import tpu as pltpu
from jax.sharding import PartitionSpec as P

HEADS = 8
CONTENT = 64
ROTARY = 32
VALUE = 64


norm_eps = 1e-06
rope_base = 10000.0


def rms_rows(entries, gain_row):
    widened = entries.astype(jnp.float32)
    return widened * lax.rsqrt(jnp.mean(widened * widened, -1, keepdims=True) + norm_eps) * gain_row


def turn_pairs(entries, positions):
    width_full = entries.shape[-1]
    frequency = rope_base ** (-jnp.arange(width_full // 2, dtype=jnp.float32) * 2.0 / width_full)
    angles = positions.astype(jnp.float32)[:, None] * frequency[None, :]
    cosine = jnp.cos(angles)[:, None, :]
    sine_part = jnp.sin(angles)[:, None, :]
    even_part = entries[..., 0::2]
    odd_part = entries[..., 1::2]
    joined = jnp.stack(
        [even_part * cosine - odd_part * sine_part, even_part * sine_part + odd_part * cosine], -1
    )
    return joined.reshape(entries.shape)


def absorb_block(carried, query_part, query_turn, key_part, key_turn, value_rows, score_scale):
    running_peak, running_total, summed = carried
    scores = jnp.einsum("qhc,khc->qhk", query_part, key_part, preferred_element_type=jnp.float32)
    scores = scores + jnp.einsum(
        "qhr,kr->qhk", query_turn, key_turn, preferred_element_type=jnp.float32
    )
    scores = scores * score_scale
    new_peak = jnp.maximum(running_peak, jnp.max(scores, -1))
    factor = jnp.exp(running_peak - new_peak)
    weights = jnp.exp(scores - new_peak[..., None])
    running_total = running_total * factor + jnp.sum(weights, -1)
    summed = summed * factor[..., None] + jnp.einsum(
        "qhk,khv->qhv", weights.astype(jnp.bfloat16), value_rows, preferred_element_type=jnp.float32
    )
    return (new_peak, running_total, summed)


def absorb_piece(carried, query_part, query_turn, key_part, key_turn, value_rows, score_scale):
    row_count = key_part.shape[0]
    key_block = math.gcd(row_count, 2048)
    if key_block == row_count:
        return absorb_block(
            carried, query_part, query_turn, key_part, key_turn, value_rows, score_scale
        )
    block_count = row_count // key_block

    def advance(state, pieces):
        return (
            absorb_block(
                state, query_part, query_turn, pieces[0], pieces[1], pieces[2], score_scale
            ),
            None,
        )

    stacked = (
        key_part.reshape((block_count, key_block) + key_part.shape[1:]),
        key_turn.reshape(block_count, key_block, key_turn.shape[1]),
        value_rows.reshape((block_count, key_block) + value_rows.shape[1:]),
    )
    carried, ignored = lax.scan(advance, carried, stacked)
    return carried


def expand_keys(latent_rows, key_columns, value_columns, head_local):
    row_count = latent_rows.shape[0]
    key_part = (
        jnp.dot(latent_rows, key_columns, preferred_element_type=jnp.float32)
        .astype(jnp.bfloat16)
        .reshape(row_count, head_local, CONTENT)
    )
    value_rows = (
        jnp.dot(latent_rows, value_columns, preferred_element_type=jnp.float32)
        .astype(jnp.bfloat16)
        .reshape(row_count, head_local, VALUE)
    )
    return (key_part, value_rows)


def expert_terms(row_block, gate_weight, up_weight, down_weight):
    gated = jnp.einsum("secd,edf->secf", row_block, gate_weight, preferred_element_type=jnp.float32)
    lifted = jnp.einsum("secd,edf->secf", row_block, up_weight, preferred_element_type=jnp.float32)
    hidden = (jax.nn.silu(gated) * lifted).astype(jnp.bfloat16)
    return jnp.einsum("secf,efd->secd", hidden, down_weight, preferred_element_type=jnp.float32)


def shared_terms(row_block, gate_weight, up_weight, down_weight):
    gated = jnp.dot(row_block, gate_weight, preferred_element_type=jnp.float32)
    lifted = jnp.dot(row_block, up_weight, preferred_element_type=jnp.float32)
    hidden = (jax.nn.silu(gated) * lifted).astype(jnp.bfloat16)
    return jnp.dot(hidden, down_weight, preferred_element_type=jnp.float32)


def shards_plain(
    query_latent,
    key_latent,
    rotary_key,
    query_gain,
    latent_gain,
    query_content,
    query_rotary,
    key_content,
    value_weight,
    output_weight,
    expert_input,
    norm_gain,
    routes,
    route_weight,
    expert_gate,
    expert_up,
    expert_down,
    shared_gate,
    shared_up,
    shared_down,
):
    group_size = lax.axis_size("tp")
    expert_groups = lax.axis_size("ep")
    own_rows = query_latent.shape[0]
    head_local = HEADS // group_size
    head_index = lax.axis_index("tp")
    group_rows_count = own_rows * group_size
    group_start = lax.axis_index("ep") * group_rows_count
    own_start = group_start + head_index * own_rows
    score_scale = (CONTENT + ROTARY) ** (-0.5)
    query_normed = rms_rows(query_latent, query_gain).astype(jnp.bfloat16)
    latent_normed = rms_rows(key_latent, latent_gain).astype(jnp.bfloat16)
    own_positions = own_start + jnp.arange(own_rows, dtype=jnp.int32)
    key_turned = turn_pairs(rotary_key.astype(jnp.float32)[:, None, :], own_positions)[
        :, 0, :
    ].astype(jnp.bfloat16)
    token_rows = expert_input.shape[0]
    picks = routes.shape[1]
    local_experts = expert_gate.shape[0]
    expert_total = local_experts * expert_groups
    capacity = 2 * token_rows * picks // expert_total
    slot_total = expert_total * capacity
    model_width = expert_input.shape[1]
    expert_normed = rms_rows(expert_input, norm_gain).astype(jnp.bfloat16)
    flat_routes = routes.reshape(-1)
    marks = (flat_routes[:, None] == jnp.arange(expert_total, dtype=jnp.int32)[None, :]).astype(
        jnp.int32
    )
    ranks = jnp.sum((jnp.cumsum(marks, 0) - marks) * marks, 1)
    targets = flat_routes * capacity + ranks
    picker = (jnp.arange(slot_total, dtype=jnp.int32)[:, None] == targets[None, :]).astype(
        jnp.int32
    )
    picker = jnp.sum(picker.reshape(slot_total, token_rows, picks), 2).astype(jnp.bfloat16)
    outgoing = jnp.dot(picker, expert_normed, preferred_element_type=jnp.float32).astype(
        jnp.bfloat16
    )
    outgoing = outgoing.reshape(expert_groups, local_experts, capacity, model_width)
    received = lax.all_to_all(outgoing, "ep", split_axis=0, concat_axis=0, tiled=True)
    group_query, group_latent, group_turn, gathered_rows, gathered_tokens = (
        lax.all_gather(query_normed, "tp", axis=0, tiled=True),
        lax.all_gather(latent_normed, "tp", axis=0, tiled=True),
        lax.all_gather(key_turned, "tp", axis=0, tiled=True),
        lax.all_gather(received, "tp", axis=0, tiled=True),
        lax.all_gather(expert_normed, "tp", axis=0, tiled=True),
    )
    positions = group_start + jnp.arange(group_rows_count, dtype=jnp.int32)
    content_columns = lax.dynamic_slice_in_dim(
        query_content, head_index * head_local * CONTENT, head_local * CONTENT, 1
    )
    rotary_columns = lax.dynamic_slice_in_dim(
        query_rotary, head_index * head_local * ROTARY, head_local * ROTARY, 1
    )
    query_part = (
        jnp.dot(group_query, content_columns, preferred_element_type=jnp.float32)
        .astype(jnp.bfloat16)
        .reshape(group_rows_count, head_local, CONTENT)
    )
    query_turn = turn_pairs(
        jnp.dot(group_query, rotary_columns, preferred_element_type=jnp.float32).reshape(
            group_rows_count, head_local, ROTARY
        ),
        positions,
    ).astype(jnp.bfloat16)
    key_columns = lax.dynamic_slice_in_dim(
        key_content, head_index * head_local * CONTENT, head_local * CONTENT, 1
    )
    value_columns = lax.dynamic_slice_in_dim(
        value_weight, head_index * head_local * VALUE, head_local * VALUE, 1
    )
    carry_start = (
        jnp.full((group_rows_count, head_local), -jnp.inf, jnp.float32),
        jnp.zeros((group_rows_count, head_local), jnp.float32),
        jnp.zeros((group_rows_count, head_local, VALUE), jnp.float32),
    )
    key_part, value_rows = expand_keys(
        lax.all_gather(group_latent, "ep", axis=0, tiled=True),
        key_columns,
        value_columns,
        head_local,
    )
    running_peak, running_total, summed = absorb_piece(
        carry_start,
        query_part,
        query_turn,
        key_part,
        lax.all_gather(group_turn, "ep", axis=0, tiled=True),
        value_rows,
        score_scale,
    )
    attended = (
        (summed / running_total[..., None])
        .astype(jnp.bfloat16)
        .reshape(group_rows_count, head_local * VALUE)
    )
    routed_term = expert_terms(gathered_rows, expert_gate, expert_up, expert_down)
    shared_term = shared_terms(gathered_tokens, shared_gate, shared_up, shared_down)
    mixer_term = jnp.dot(attended, output_weight, preferred_element_type=jnp.float32)
    mixer_sum, routed_sum, shared_sum = (
        lax.psum_scatter(
            mixer_term.astype(jnp.bfloat16), "tp", scatter_dimension=0, tiled=True
        ).astype(jnp.float32),
        lax.psum_scatter(
            routed_term.astype(jnp.bfloat16), "tp", scatter_dimension=0, tiled=True
        ).astype(jnp.float32),
        lax.psum_scatter(
            shared_term.astype(jnp.bfloat16), "tp", scatter_dimension=0, tiled=True
        ).astype(jnp.float32),
    )
    mixer_out = mixer_sum.astype(jnp.bfloat16)
    returned = lax.all_to_all(
        routed_sum.astype(jnp.bfloat16), "ep", split_axis=0, concat_axis=0, tiled=True
    )
    returned = returned.reshape(slot_total, model_width)
    picked = jnp.take(returned, targets, axis=0).reshape(token_rows, picks, model_width)
    combined = jnp.sum(route_weight[..., None] * picked.astype(jnp.float32), 1) + shared_sum
    expert_out = combined.astype(jnp.bfloat16)
    return (mixer_out, expert_out)


MESH = pl.DeviceIdType.MESH
VMEM_LIMIT = 60 * 1024 * 1024


def greet(ep_count, me, head_index):
    barrier = pltpu.get_barrier_semaphore()
    for step in range(1, ep_count):
        pl.semaphore_signal(
            barrier, inc=1, device_id=(lax.rem(me + step, ep_count), head_index), device_id_type=MESH
        )
    row, core = head_index // 2, head_index % 2
    for other in ((1 - row) * 2 + core, row * 2 + 1 - core):
        pl.semaphore_signal(barrier, inc=1, device_id=(me, other), device_id_type=MESH)
    pl.semaphore_wait(barrier, ep_count + 1)


def gated_rows(rows, gate_weight, up_weight):
    gated = jnp.dot(rows, gate_weight, preferred_element_type=jnp.float32)
    lifted = jnp.dot(rows, up_weight, preferred_element_type=jnp.float32)
    return (gated / (1.0 + jnp.exp(-gated)) * lifted).astype(jnp.bfloat16)


def block_kernel(
    ep_count,
    capacity,
    slots_ref,
    latent_ref,
    tokens_ref,
    query_ref,
    query_columns_ref,
    latent_columns_ref,
    turns_ref,
    output_weight_ref,
    weight_ref,
    gate_hbm,
    up_hbm,
    down_hbm,
    shared_gate_hbm,
    shared_up_hbm,
    shared_down_hbm,
    mixer_out,
    expert_out,
    rows,
    latents,
    tokens,
    queries,
    gate_ref,
    up_ref,
    down_ref,
    shared_gate_ref,
    shared_up_ref,
    shared_down_ref,
    keys,
    values,
    query_wide,
    attended,
    part,
    side,
    half_rows,
    half_side,
    far_rows,
    far_side,
    returned,
    ep_send,
    ep_recv,
    y_send,
    y_recv,
    core_send,
    core_recv,
    cross_send,
    cross_recv,
    own_sem,
    weight_sem,
    half_send,
    half_recv,
    far_send,
    far_recv,
    back_send,
    back_recv,
):
    me = lax.axis_index("ep")
    head_index = lax.axis_index("tp")
    row, core = head_index // 2, head_index % 2
    y_peer = (me, (1 - row) * 2 + core)
    core_peer = (me, row * 2 + 1 - core)
    local_experts = gate_ref.shape[0]
    width = rows.shape[-1]
    own_rows = tokens.shape[2]
    slot_rows = rows.shape[3]
    stripe = math.gcd(width, 512)

    def remote(source, target, send_sem, recv_sem, device):
        return pltpu.make_async_remote_copy(
            src_ref=source,
            dst_ref=target,
            send_sem=send_sem,
            recv_sem=recv_sem,
            device_id=device,
            device_id_type=MESH,
        )

    fetches = [
        pltpu.make_async_copy(source, target, weight_sem.at[place])
        for place, (source, target) in enumerate(
            (
                (shared_gate_hbm, shared_gate_ref),
                (shared_up_hbm, shared_up_ref),
                (shared_down_hbm, shared_down_ref),
                (gate_hbm, gate_ref),
                (up_hbm, up_ref),
                (down_hbm, down_ref),
            )
        )
    ]
    own = (
        pltpu.make_async_copy(latent_ref, latents.at[row, core, 0], own_sem.at[0]),
        pltpu.make_async_copy(slots_ref.at[me], rows.at[row, core, 0], own_sem.at[1]),
        pltpu.make_async_copy(tokens_ref, tokens.at[row, core], own_sem.at[2]),
        pltpu.make_async_copy(query_ref, queries.at[row, core], own_sem.at[3]),
    )
    for copy in own:
        copy.start()
    greet(ep_count, me, head_index)

    def latent_ep(step):
        return remote(
            latent_ref,
            latents.at[row, core, step],
            ep_send.at[1, step],
            ep_recv.at[1, step],
            (lax.rem(me + step, ep_count), head_index),
        )

    def slots_ep(step):
        peer = lax.rem(me + step, ep_count)
        return remote(
            slots_ref.at[peer],
            rows.at[row, core, step],
            ep_send.at[0, step],
            ep_recv.at[0, step],
            (peer, head_index),
        )

    routes_of = {
        "y": (row, y_send, y_recv, y_peer),
        "core": (row, core_send, core_recv, core_peer),
        "cross": (1 - row, cross_send, cross_recv, core_peer),
    }

    def moved(buffer, place, step, route):
        origin_row, send_sem, recv_sem, device = routes_of[route]
        block = buffer.at[origin_row, core] if step == ep_count else buffer.at[origin_row, core, step]
        return remote(block, block, send_sem.at[place, step], recv_sem.at[place, step], device)

    for step in range(1, ep_count):
        latent_ep(step).start()
    for step in range(1, ep_count):
        slots_ep(step).start()
    for copy in own:
        copy.wait()
    for route in ("y", "core"):
        moved(queries, 1, ep_count, route).start()
        moved(latents, 1, 0, route).start()
        moved(tokens, 0, ep_count, route).start()
    for fetch in fetches:
        fetch.start()
    for step in range(1, ep_count):
        latent_ep(step).wait_recv()
        for route in ("y", "core"):
            moved(latents, 1, step, route).start()
    moved(queries, 1, ep_count, "y").wait_recv()
    moved(queries, 1, ep_count, "cross").start()
    moved(tokens, 0, ep_count, "y").wait_recv()
    moved(tokens, 0, ep_count, "cross").start()
    for route in ("y", "core"):
        moved(rows, 0, 0, route).start()
    for step in range(ep_count):
        moved(latents, 1, step, "y").wait_recv()
        moved(latents, 1, step, "cross").start()
    for route in ("core", "cross"):
        moved(queries, 1, ep_count, route).wait_recv()
        for step in range(ep_count):
            moved(latents, 1, step, route).wait_recv()

    rank_width = latent_columns_ref.shape[0]
    head_lanes = attended.shape[1]
    group_rows = attended.shape[0]
    heads = head_lanes // VALUE

    def project():
        query_rows = queries[...].reshape(group_rows, queries.shape[-1])
        projected = jnp.dot(
            query_rows, query_columns_ref[...], preferred_element_type=jnp.float32
        )
        query_wide[:, :head_lanes] = projected[:, :head_lanes].astype(jnp.bfloat16)
        turned = (
            projected[:, head_lanes : head_lanes + 128] * turns_ref[0]
            + projected[:, head_lanes + 128 :] * turns_ref[1]
        )
        query_wide[:, head_lanes:] = turned.astype(jnp.bfloat16)
        for block in range(4):
            packed = latents[block // 2, block % 2].reshape(ep_count * own_rows, latents.shape[-1])
            expanded = jnp.dot(
                packed[:, :rank_width],
                latent_columns_ref[...],
                preferred_element_type=jnp.float32,
            ).astype(jnp.bfloat16)
            span = slice(block * ep_count * own_rows, (block + 1) * ep_count * own_rows)
            keys[span, :head_lanes] = expanded[:, :head_lanes]
            keys[span, head_lanes:] = packed[:, rank_width:]
            values[span, :] = expanded[:, head_lanes:]

    def attend(block):
        block_rows = group_rows // 4
        span = slice(block * block_rows, (block + 1) * block_rows)
        query_block = query_wide[span, :]
        lane = lax.broadcasted_iota(jnp.int32, query_block.shape, 1)
        lane_head = jnp.where(lane < head_lanes, lane // CONTENT, (lane - head_lanes) // ROTARY)
        out_lane = lax.broadcasted_iota(jnp.int32, (block_rows, head_lanes), 1)
        result = jnp.zeros((block_rows, head_lanes), jnp.float32)
        for head in range(heads):
            chosen = jnp.where(lane_head == head, query_block, jnp.zeros_like(query_block))
            scores = lax.dot_general(
                chosen, keys[...], (((1,), (1,)), ((), ())), preferred_element_type=jnp.float32
            ) * ((CONTENT + ROTARY) ** (-0.5))
            weights = jnp.exp(scores - jnp.max(scores, -1, keepdims=True))
            total = jnp.sum(weights, -1, keepdims=True)
            summed = jnp.dot(
                weights.astype(jnp.bfloat16), values[...], preferred_element_type=jnp.float32
            )
            result = jnp.where(out_lane // VALUE == head, summed / total, result)
        attended[span, :] = result.astype(jnp.bfloat16)

    def mix():
        for start in range(0, width, stripe):
            product = jnp.dot(
                attended[...],
                output_weight_ref[:, start : start + stripe],
                preferred_element_type=jnp.float32,
            ).astype(jnp.bfloat16)
            side[:, :, own_rows:, start : start + stripe] = product.reshape(
                2, 2, own_rows, stripe
            )

    def share():
        for fetch in fetches[:3]:
            fetch.wait()
        for route in ("core", "cross"):
            moved(tokens, 0, ep_count, route).wait_recv()
        hidden = gated_rows(
            tokens[...].reshape(group_rows, width), shared_gate_ref[...], shared_up_ref[...]
        )
        for start in range(0, width, stripe):
            product = jnp.dot(
                hidden,
                shared_down_ref[:, start : start + stripe],
                preferred_element_type=jnp.float32,
            ).astype(jnp.bfloat16)
            side[:, :, :own_rows, start : start + stripe] = product.reshape(
                2, 2, own_rows, stripe
            )

    def side_half(target_row, place):
        return remote(
            side.at[target_row, 1 - core],
            half_side.at[target_row],
            half_send.at[1, place],
            half_recv.at[1, place],
            core_peer,
        )

    near_side, outer_side = side_half(row, 0), side_half(1 - row, 1)
    side_copy = remote(
        side.at[1 - row, core], far_side, far_send.at[ep_count], far_recv.at[ep_count], y_peer
    )

    def side_exchange():
        outer_side.start()
        near_side.start()

    def side_far():
        outer_side.wait_recv()
        side[1 - row, core] = (
            side[1 - row, core].astype(jnp.float32) + half_side[1 - row].astype(jnp.float32)
        ).astype(jnp.bfloat16)

    tasks = [
        project,
        lambda: attend(0),
        lambda: attend(1),
        lambda: attend(2),
        lambda: attend(3),
        mix,
        share,
        side_exchange,
        side_far,
    ]
    for step in range(max(ep_count + 1, len(tasks))):
        if 0 < step < ep_count:
            slots_ep(step).wait_recv()
            for route in ("y", "core"):
                moved(rows, 0, step, route).start()
        if 0 < step <= ep_count:
            moved(rows, 0, step - 1, "y").wait_recv()
            moved(rows, 0, step - 1, "cross").start()
        if step < len(tasks):
            tasks[step]()
    side_copy.start()
    for fetch in fetches[3:]:
        fetch.wait()
    for route in ("core", "cross"):
        for step in range(ep_count):
            moved(rows, 0, step, route).wait_recv()

    def compute(side_core):
        for expert in range(local_experts):
            span = slice(expert * capacity, (expert + 1) * capacity)
            block = rows[:, side_core, :, span, :].reshape(2 * ep_count * capacity, width)
            hidden = gated_rows(block, gate_ref[expert], up_ref[expert])
            for start in range(0, width, stripe):
                product = jnp.dot(
                    hidden,
                    down_ref[expert, :, start : start + stripe],
                    preferred_element_type=jnp.float32,
                ).astype(jnp.bfloat16)
                part[:, side_core, :, span, start : start + stripe] = product.reshape(
                    2, ep_count, capacity, stripe
                )

    def rows_half(target_row, place):
        return remote(
            part.at[target_row, 1 - core],
            half_rows.at[target_row],
            half_send.at[0, place],
            half_recv.at[0, place],
            core_peer,
        )

    compute(1 - core)
    near, outer = rows_half(row, 0), rows_half(1 - row, 1)
    outer.start()
    near.start()
    compute(core)

    def y_copy(step):
        return remote(
            part.at[1 - row, core, step],
            far_rows.at[step],
            far_send.at[step],
            far_recv.at[step],
            y_peer,
        )

    def back_copy(step):
        return remote(
            part.at[row, core, step],
            returned.at[me],
            back_send.at[step],
            back_recv.at[step],
            (lax.rem(me + ep_count - step, ep_count), head_index),
        )

    outer.wait_recv()
    order = list(range(1, ep_count)) + [0]
    for step in order:
        part[1 - row, core, step] = (
            part[1 - row, core, step].astype(jnp.float32)
            + half_rows[1 - row, step].astype(jnp.float32)
        ).astype(jnp.bfloat16)
        y_copy(step).start()
    near.wait_recv()
    near_side.wait_recv()
    side_copy.wait_recv()
    side_total = (
        side[row, core].astype(jnp.float32)
        + half_side[row].astype(jnp.float32)
        + far_side[...].astype(jnp.float32)
    )
    mixer_out[...] = side_total[own_rows:].astype(jnp.bfloat16)
    for step in order:
        y_copy(step).wait_recv()
        total = (
            part[row, core, step].astype(jnp.float32)
            + half_rows[row, step].astype(jnp.float32)
            + far_rows[step].astype(jnp.float32)
        ).astype(jnp.bfloat16)
        if step > 0:
            part[row, core, step] = total
            back_copy(step).start()
        else:
            returned[me] = total
    for step in range(1, ep_count):
        back_copy(step).wait_recv()
    for start in range(0, width, stripe):
        picked = jnp.dot(
            weight_ref[...],
            returned[:, :, start : start + stripe].reshape(ep_count * slot_rows, stripe),
            preferred_element_type=jnp.float32,
        )
        picked = picked[:own_rows] + picked[own_rows : 2 * own_rows] + picked[2 * own_rows :]
        expert_out[:, start : start + stripe] = (
            picked + side_total[:own_rows, start : start + stripe]
        ).astype(jnp.bfloat16)

    for step in range(1, ep_count):
        latent_ep(step).wait_send()
        slots_ep(step).wait_send()
        back_copy(step).wait_send()
    for route in ("y", "core", "cross"):
        moved(queries, 1, ep_count, route).wait_send()
        moved(tokens, 0, ep_count, route).wait_send()
        for step in range(ep_count):
            moved(latents, 1, step, route).wait_send()
            moved(rows, 0, step, route).wait_send()
    for copy in (near, outer, near_side, outer_side, side_copy):
        copy.wait_send()
    for step in range(ep_count):
        y_copy(step).wait_send()


def block_call(capacity, *operands):
    slots, latent_pack, tokens, queries = operands[:4]
    ep_count, slot_rows, width = slots.shape
    own_rows = tokens.shape[0]
    head_lanes = operands[7].shape[0]
    vmem = pl.BlockSpec(memory_space=pltpu.VMEM)
    anywhere = pl.BlockSpec(memory_space=pl.ANY)
    out = jax.ShapeDtypeStruct((own_rows, width), jnp.bfloat16)

    def held(*shape):
        return pltpu.VMEM(shape, jnp.bfloat16)

    def sems(*shape):
        return pltpu.SemaphoreType.DMA(shape)

    key_rows = 4 * ep_count * own_rows
    return pl.pallas_call(
        lambda *refs: block_kernel(ep_count, capacity, *refs),
        out_shape=(out, out),
        in_specs=[vmem] * 9 + [anywhere] * 6,
        out_specs=(vmem, vmem),
        scratch_shapes=[
            held(2, 2, ep_count, slot_rows, width),
            held(2, 2, ep_count, *latent_pack.shape),
            held(2, 2, *tokens.shape),
            held(2, 2, *queries.shape),
        ]
        + [held(*operand.shape) for operand in operands[9:]]
        + [
            held(key_rows, head_lanes + 128),
            held(key_rows, head_lanes),
            held(4 * own_rows, head_lanes + 128),
            held(4 * own_rows, head_lanes),
            held(2, 2, ep_count, slot_rows, width),
            held(2, 2, 2 * own_rows, width),
            held(2, ep_count, slot_rows, width),
            held(2, 2 * own_rows, width),
            held(ep_count, slot_rows, width),
            held(2 * own_rows, width),
            held(ep_count, slot_rows, width),
        ]
        + [sems(2, ep_count + 1)] * 8
        + [
            sems(4),
            sems(6),
            sems(2, 2),
            sems(2, 2),
            sems(ep_count + 1),
            sems(ep_count + 1),
            sems(ep_count),
            sems(ep_count),
        ],
        compiler_params=pltpu.CompilerParams(
            collective_id=0, has_side_effects=True, vmem_limit_bytes=VMEM_LIMIT
        ),
        name="block",
    )(*operands)


def shards(
    query_latent,
    key_latent,
    rotary_key,
    query_gain,
    latent_gain,
    query_content,
    query_rotary,
    key_content,
    value_weight,
    output_weight,
    expert_input,
    norm_gain,
    routes,
    route_weight,
    expert_gate,
    expert_up,
    expert_down,
    shared_gate,
    shared_up,
    shared_down,
):
    group_size = lax.axis_size("tp")
    expert_groups = lax.axis_size("ep")
    token_rows = expert_input.shape[0]
    picks = routes.shape[1]
    local_experts = expert_gate.shape[0]
    expert_total = local_experts * expert_groups
    capacity = 2 * token_rows * picks // expert_total
    if group_size != 4 or capacity % 16:
        return shards_plain(
            query_latent,
            key_latent,
            rotary_key,
            query_gain,
            latent_gain,
            query_content,
            query_rotary,
            key_content,
            value_weight,
            output_weight,
            expert_input,
            norm_gain,
            routes,
            route_weight,
            expert_gate,
            expert_up,
            expert_down,
            shared_gate,
            shared_up,
            shared_down,
        )
    own_rows = query_latent.shape[0]
    head_local = HEADS // group_size
    head_index = lax.axis_index("tp")
    group_rows_count = own_rows * group_size
    group_start = lax.axis_index("ep") * group_rows_count
    own_start = group_start + head_index * own_rows
    score_scale = (CONTENT + ROTARY) ** (-0.5)
    query_normed = rms_rows(query_latent, query_gain).astype(jnp.bfloat16)
    latent_normed = rms_rows(key_latent, latent_gain).astype(jnp.bfloat16)
    own_positions = own_start + jnp.arange(own_rows, dtype=jnp.int32)
    key_turned = turn_pairs(rotary_key.astype(jnp.float32)[:, None, :], own_positions)[
        :, 0, :
    ].astype(jnp.bfloat16)
    slot_total = expert_total * capacity
    model_width = expert_input.shape[1]
    expert_normed = rms_rows(expert_input, norm_gain).astype(jnp.bfloat16)
    flat_routes = routes.reshape(-1)
    marks = (flat_routes[:, None] == jnp.arange(expert_total, dtype=jnp.int32)[None, :]).astype(
        jnp.int32
    )
    ranks = jnp.sum((jnp.cumsum(marks, 0) - marks) * marks, 1)
    targets = (flat_routes * capacity + ranks).reshape(token_rows, picks)
    chosen = targets[:, :, None] == jnp.arange(slot_total, dtype=jnp.int32)[None, None, :]
    picker = jnp.any(chosen, 1).astype(jnp.bfloat16)
    spread_weight = jnp.sum(jnp.where(chosen, route_weight[:, :, None], 0.0), 1)
    high = lax.reduce_precision(spread_weight, 8, 7)
    middle = lax.reduce_precision(spread_weight - high, 8, 7)
    low = spread_weight - high - middle
    weight_terms = jnp.concatenate([high, middle, low], 0).astype(jnp.bfloat16)
    slots = lax.dot_general(
        picker, expert_normed, (((0,), (0,)), ((), ())), preferred_element_type=jnp.float32
    ).astype(jnp.bfloat16)
    slots = slots.reshape(expert_groups, local_experts * capacity, model_width)
    latent_pack = jnp.concatenate(
        [latent_normed]
        + [key_turned] * head_local
        + [jnp.zeros((own_rows, -head_local * ROTARY % 128), jnp.bfloat16)],
        1,
    )
    content_columns = lax.dynamic_slice_in_dim(
        query_content, head_index * head_local * CONTENT, head_local * CONTENT, 1
    )
    rotary_columns = lax.dynamic_slice_in_dim(
        query_rotary, head_index * head_local * ROTARY, head_local * ROTARY, 1
    )
    paired = rotary_columns.reshape(-1, head_local * ROTARY // 2, 2)
    swapped_columns = jnp.stack([-paired[:, :, 1], paired[:, :, 0]], -1).reshape(
        rotary_columns.shape
    )
    lane_pad = ((0, 0), (0, -head_local * ROTARY % 128))
    query_columns = jnp.concatenate(
        [content_columns, jnp.pad(rotary_columns, lane_pad), jnp.pad(swapped_columns, lane_pad)], 1
    )
    key_columns = lax.dynamic_slice_in_dim(
        key_content, head_index * head_local * CONTENT, head_local * CONTENT, 1
    )
    value_columns = lax.dynamic_slice_in_dim(
        value_weight, head_index * head_local * VALUE, head_local * VALUE, 1
    )
    latent_columns = jnp.concatenate([key_columns, value_columns], 1)
    positions = group_start + jnp.arange(group_rows_count, dtype=jnp.int32)
    frequency = rope_base ** (-jnp.arange(ROTARY // 2, dtype=jnp.float32) * 2.0 / ROTARY)
    angles = positions.astype(jnp.float32)[:, None] * jnp.tile(
        jnp.repeat(frequency, 2), 128 // ROTARY
    )[None, :]
    turns = jnp.stack([jnp.cos(angles), jnp.sin(angles)])
    return block_call(
        capacity,
        slots,
        latent_pack,
        expert_normed,
        query_normed,
        query_columns,
        latent_columns,
        turns,
        output_weight,
        weight_terms,
        expert_gate,
        expert_up,
        expert_down,
        shared_gate,
        shared_up,
        shared_down,
    )


def solution(mesh):
    in_specs = (
        P(("ep", "tp"), None),
        P(("ep", "tp"), None),
        P(("ep", "tp"), None),
        P(),
        P(),
        P(),
        P(),
        P(),
        P(),
        P("tp", None),
        P(("ep", "tp"), None),
        P(),
        P(("ep", "tp"), None),
        P(("ep", "tp"), None),
        P("ep", None, "tp"),
        P("ep", None, "tp"),
        P("ep", "tp", None),
        P(None, "tp"),
        P(None, "tp"),
        P("tp", None),
    )
    out_specs = (P(("ep", "tp"), None), P(("ep", "tp"), None))
    return jax.shard_map(shards, mesh=mesh, in_specs=in_specs, out_specs=out_specs, check_vma=False)
```

```python
import math

import jax
import jax.numpy as jnp
from jax import lax
from jax.experimental import pallas as pl
from jax.experimental.pallas import tpu as pltpu
from jax.sharding import PartitionSpec as P

HEADS = 8
CONTENT = 64
ROTARY = 32
VALUE = 64


norm_eps = 1e-06
rope_base = 10000.0


def rms_rows(entries, gain_row):
    widened = entries.astype(jnp.float32)
    return widened * lax.rsqrt(jnp.mean(widened * widened, -1, keepdims=True) + norm_eps) * gain_row


def turn_pairs(entries, positions):
    width_full = entries.shape[-1]
    frequency = rope_base ** (-jnp.arange(width_full // 2, dtype=jnp.float32) * 2.0 / width_full)
    angles = positions.astype(jnp.float32)[:, None] * frequency[None, :]
    cosine = jnp.cos(angles)[:, None, :]
    sine_part = jnp.sin(angles)[:, None, :]
    even_part = entries[..., 0::2]
    odd_part = entries[..., 1::2]
    joined = jnp.stack(
        [even_part * cosine - odd_part * sine_part, even_part * sine_part + odd_part * cosine], -1
    )
    return joined.reshape(entries.shape)


def absorb_block(carried, query_part, query_turn, key_part, key_turn, value_rows, score_scale):
    running_peak, running_total, summed = carried
    scores = jnp.einsum("qhc,khc->qhk", query_part, key_part, preferred_element_type=jnp.float32)
    scores = scores + jnp.einsum(
        "qhr,kr->qhk", query_turn, key_turn, preferred_element_type=jnp.float32
    )
    scores = scores * score_scale
    new_peak = jnp.maximum(running_peak, jnp.max(scores, -1))
    factor = jnp.exp(running_peak - new_peak)
    weights = jnp.exp(scores - new_peak[..., None])
    running_total = running_total * factor + jnp.sum(weights, -1)
    summed = summed * factor[..., None] + jnp.einsum(
        "qhk,khv->qhv", weights.astype(jnp.bfloat16), value_rows, preferred_element_type=jnp.float32
    )
    return (new_peak, running_total, summed)


def absorb_piece(carried, query_part, query_turn, key_part, key_turn, value_rows, score_scale):
    row_count = key_part.shape[0]
    key_block = math.gcd(row_count, 2048)
    if key_block == row_count:
        return absorb_block(
            carried, query_part, query_turn, key_part, key_turn, value_rows, score_scale
        )
    block_count = row_count // key_block

    def advance(state, pieces):
        return (
            absorb_block(
                state, query_part, query_turn, pieces[0], pieces[1], pieces[2], score_scale
            ),
            None,
        )

    stacked = (
        key_part.reshape((block_count, key_block) + key_part.shape[1:]),
        key_turn.reshape(block_count, key_block, key_turn.shape[1]),
        value_rows.reshape((block_count, key_block) + value_rows.shape[1:]),
    )
    carried, ignored = lax.scan(advance, carried, stacked)
    return carried


def expand_keys(latent_rows, key_columns, value_columns, head_local):
    row_count = latent_rows.shape[0]
    key_part = (
        jnp.dot(latent_rows, key_columns, preferred_element_type=jnp.float32)
        .astype(jnp.bfloat16)
        .reshape(row_count, head_local, CONTENT)
    )
    value_rows = (
        jnp.dot(latent_rows, value_columns, preferred_element_type=jnp.float32)
        .astype(jnp.bfloat16)
        .reshape(row_count, head_local, VALUE)
    )
    return (key_part, value_rows)


def expert_terms(row_block, gate_weight, up_weight, down_weight):
    gated = jnp.einsum("secd,edf->secf", row_block, gate_weight, preferred_element_type=jnp.float32)
    lifted = jnp.einsum("secd,edf->secf", row_block, up_weight, preferred_element_type=jnp.float32)
    hidden = (jax.nn.silu(gated) * lifted).astype(jnp.bfloat16)
    return jnp.einsum("secf,efd->secd", hidden, down_weight, preferred_element_type=jnp.float32)


def shared_terms(row_block, gate_weight, up_weight, down_weight):
    gated = jnp.dot(row_block, gate_weight, preferred_element_type=jnp.float32)
    lifted = jnp.dot(row_block, up_weight, preferred_element_type=jnp.float32)
    hidden = (jax.nn.silu(gated) * lifted).astype(jnp.bfloat16)
    return jnp.dot(hidden, down_weight, preferred_element_type=jnp.float32)


def shards_plain(
    query_latent,
    key_latent,
    rotary_key,
    query_gain,
    latent_gain,
    query_content,
    query_rotary,
    key_content,
    value_weight,
    output_weight,
    expert_input,
    norm_gain,
    routes,
    route_weight,
    expert_gate,
    expert_up,
    expert_down,
    shared_gate,
    shared_up,
    shared_down,
):
    group_size = lax.axis_size("tp")
    expert_groups = lax.axis_size("ep")
    own_rows = query_latent.shape[0]
    head_local = HEADS // group_size
    head_index = lax.axis_index("tp")
    group_rows_count = own_rows * group_size
    group_start = lax.axis_index("ep") * group_rows_count
    own_start = group_start + head_index * own_rows
    score_scale = (CONTENT + ROTARY) ** (-0.5)
    query_normed = rms_rows(query_latent, query_gain).astype(jnp.bfloat16)
    latent_normed = rms_rows(key_latent, latent_gain).astype(jnp.bfloat16)
    own_positions = own_start + jnp.arange(own_rows, dtype=jnp.int32)
    key_turned = turn_pairs(rotary_key.astype(jnp.float32)[:, None, :], own_positions)[
        :, 0, :
    ].astype(jnp.bfloat16)
    token_rows = expert_input.shape[0]
    picks = routes.shape[1]
    local_experts = expert_gate.shape[0]
    expert_total = local_experts * expert_groups
    capacity = 2 * token_rows * picks // expert_total
    slot_total = expert_total * capacity
    model_width = expert_input.shape[1]
    expert_normed = rms_rows(expert_input, norm_gain).astype(jnp.bfloat16)
    flat_routes = routes.reshape(-1)
    marks = (flat_routes[:, None] == jnp.arange(expert_total, dtype=jnp.int32)[None, :]).astype(
        jnp.int32
    )
    ranks = jnp.sum((jnp.cumsum(marks, 0) - marks) * marks, 1)
    targets = flat_routes * capacity + ranks
    picker = (jnp.arange(slot_total, dtype=jnp.int32)[:, None] == targets[None, :]).astype(
        jnp.int32
    )
    picker = jnp.sum(picker.reshape(slot_total, token_rows, picks), 2).astype(jnp.bfloat16)
    outgoing = jnp.dot(picker, expert_normed, preferred_element_type=jnp.float32).astype(
        jnp.bfloat16
    )
    outgoing = outgoing.reshape(expert_groups, local_experts, capacity, model_width)
    received = lax.all_to_all(outgoing, "ep", split_axis=0, concat_axis=0, tiled=True)
    group_query, group_latent, group_turn, gathered_rows, gathered_tokens = (
        lax.all_gather(query_normed, "tp", axis=0, tiled=True),
        lax.all_gather(latent_normed, "tp", axis=0, tiled=True),
        lax.all_gather(key_turned, "tp", axis=0, tiled=True),
        lax.all_gather(received, "tp", axis=0, tiled=True),
        lax.all_gather(expert_normed, "tp", axis=0, tiled=True),
    )
    positions = group_start + jnp.arange(group_rows_count, dtype=jnp.int32)
    content_columns = lax.dynamic_slice_in_dim(
        query_content, head_index * head_local * CONTENT, head_local * CONTENT, 1
    )
    rotary_columns = lax.dynamic_slice_in_dim(
        query_rotary, head_index * head_local * ROTARY, head_local * ROTARY, 1
    )
    query_part = (
        jnp.dot(group_query, content_columns, preferred_element_type=jnp.float32)
        .astype(jnp.bfloat16)
        .reshape(group_rows_count, head_local, CONTENT)
    )
    query_turn = turn_pairs(
        jnp.dot(group_query, rotary_columns, preferred_element_type=jnp.float32).reshape(
            group_rows_count, head_local, ROTARY
        ),
        positions,
    ).astype(jnp.bfloat16)
    key_columns = lax.dynamic_slice_in_dim(
        key_content, head_index * head_local * CONTENT, head_local * CONTENT, 1
    )
    value_columns = lax.dynamic_slice_in_dim(
        value_weight, head_index * head_local * VALUE, head_local * VALUE, 1
    )
    carry_start = (
        jnp.full((group_rows_count, head_local), -jnp.inf, jnp.float32),
        jnp.zeros((group_rows_count, head_local), jnp.float32),
        jnp.zeros((group_rows_count, head_local, VALUE), jnp.float32),
    )
    key_part, value_rows = expand_keys(
        lax.all_gather(group_latent, "ep", axis=0, tiled=True),
        key_columns,
        value_columns,
        head_local,
    )
    running_peak, running_total, summed = absorb_piece(
        carry_start,
        query_part,
        query_turn,
        key_part,
        lax.all_gather(group_turn, "ep", axis=0, tiled=True),
        value_rows,
        score_scale,
    )
    attended = (
        (summed / running_total[..., None])
        .astype(jnp.bfloat16)
        .reshape(group_rows_count, head_local * VALUE)
    )
    routed_term = expert_terms(gathered_rows, expert_gate, expert_up, expert_down)
    shared_term = shared_terms(gathered_tokens, shared_gate, shared_up, shared_down)
    mixer_term = jnp.dot(attended, output_weight, preferred_element_type=jnp.float32)
    mixer_sum, routed_sum, shared_sum = (
        lax.psum_scatter(
            mixer_term.astype(jnp.bfloat16), "tp", scatter_dimension=0, tiled=True
        ).astype(jnp.float32),
        lax.psum_scatter(
            routed_term.astype(jnp.bfloat16), "tp", scatter_dimension=0, tiled=True
        ).astype(jnp.float32),
        lax.psum_scatter(
            shared_term.astype(jnp.bfloat16), "tp", scatter_dimension=0, tiled=True
        ).astype(jnp.float32),
    )
    mixer_out = mixer_sum.astype(jnp.bfloat16)
    returned = lax.all_to_all(
        routed_sum.astype(jnp.bfloat16), "ep", split_axis=0, concat_axis=0, tiled=True
    )
    returned = returned.reshape(slot_total, model_width)
    picked = jnp.take(returned, targets, axis=0).reshape(token_rows, picks, model_width)
    combined = jnp.sum(route_weight[..., None] * picked.astype(jnp.float32), 1) + shared_sum
    expert_out = combined.astype(jnp.bfloat16)
    return (mixer_out, expert_out)


MESH = pl.DeviceIdType.MESH
VMEM_LIMIT = 60 * 1024 * 1024


def greet(ep_count, me, head_index):
    barrier = pltpu.get_barrier_semaphore()
    for step in range(1, ep_count):
        pl.semaphore_signal(
            barrier, inc=1, device_id=(lax.rem(me + step, ep_count), head_index), device_id_type=MESH
        )
    row, core = head_index // 2, head_index % 2
    for other in ((1 - row) * 2 + core, row * 2 + 1 - core):
        pl.semaphore_signal(barrier, inc=1, device_id=(me, other), device_id_type=MESH)
    pl.semaphore_wait(barrier, ep_count + 1)


def gated_rows(rows, gate_weight, up_weight):
    gated = jnp.dot(rows, gate_weight, preferred_element_type=jnp.float32)
    lifted = jnp.dot(rows, up_weight, preferred_element_type=jnp.float32)
    return (gated / (1.0 + jnp.exp(-gated)) * lifted).astype(jnp.bfloat16)


def block_kernel(
    ep_count,
    capacity,
    query_latent_ref,
    key_latent_ref,
    rotary_key_ref,
    query_gain_ref,
    latent_gain_ref,
    expert_input_ref,
    norm_gain_ref,
    routes_ref,
    route_weight_ref,
    cosine_ref,
    sine_ref,
    query_content_hbm,
    query_rotary_hbm,
    key_content_hbm,
    value_weight_hbm,
    output_weight_hbm,
    gate_hbm,
    up_hbm,
    down_hbm,
    shared_gate_hbm,
    shared_up_hbm,
    shared_down_hbm,
    both_out,
    slots_ref,
    query_columns_ref,
    latent_columns_ref,
    output_weight_ref,
    weight_ref,
    rows,
    latents,
    tokens,
    queries,
    gate_ref,
    up_ref,
    down_ref,
    shared_gate_ref,
    shared_up_ref,
    shared_down_ref,
    keys,
    values,
    query_wide,
    attended,
    part,
    side,
    half_rows,
    half_side,
    far_rows,
    far_side,
    returned,
    ep_send,
    ep_recv,
    y_send,
    y_recv,
    core_send,
    core_recv,
    cross_send,
    cross_recv,
    own_sem,
    weight_sem,
    half_send,
    half_recv,
    far_send,
    far_recv,
    back_send,
    back_recv,
):
    me = lax.axis_index("ep")
    head_index = lax.axis_index("tp")
    row, core = head_index // 2, head_index % 2
    y_peer = (me, (1 - row) * 2 + core)
    core_peer = (me, row * 2 + 1 - core)
    local_experts = gate_ref.shape[0]
    width = rows.shape[-1]
    own_rows = tokens.shape[2]
    slot_rows = rows.shape[3]
    stripe = math.gcd(width, 512)

    def remote(source, target, send_sem, recv_sem, device):
        return pltpu.make_async_remote_copy(
            src_ref=source,
            dst_ref=target,
            send_sem=send_sem,
            recv_sem=recv_sem,
            device_id=device,
            device_id_type=MESH,
        )

    head_lanes = attended.shape[1]
    heads = head_lanes // VALUE
    columns = pl.ds(pl.multiple_of(head_index * head_lanes, head_lanes), head_lanes)
    turn_columns = pl.ds(pl.multiple_of(head_index * heads * ROTARY // 128 * 128, 128), 128)
    fetches = [
        pltpu.make_async_copy(source, target, weight_sem.at[place])
        for place, (source, target) in enumerate(
            (
                (query_content_hbm.at[:, columns], query_columns_ref.at[:, :head_lanes]),
                (query_rotary_hbm.at[:, turn_columns], query_columns_ref.at[:, head_lanes:]),
                (key_content_hbm.at[:, columns], latent_columns_ref.at[:, :head_lanes]),
                (value_weight_hbm.at[:, columns], latent_columns_ref.at[:, head_lanes:]),
                (output_weight_hbm, output_weight_ref),
                (shared_gate_hbm, shared_gate_ref),
                (shared_up_hbm, shared_up_ref),
                (shared_down_hbm, shared_down_ref),
                (gate_hbm, gate_ref),
                (up_hbm, up_ref),
                (down_hbm, down_ref),
            )
        )
    ]
    for fetch in fetches:
        fetch.start()

    def turn(entries, cosine, sine):
        lane = lax.broadcasted_iota(jnp.int32, entries.shape, 1)
        crossed = jnp.where(
            lane % 2 == 0, -pltpu.roll(entries, 127, 1), pltpu.roll(entries, 1, 1)
        )
        return (entries * cosine + crossed * sine).astype(jnp.bfloat16)

    latents[row, core, 0, :, : key_latent_ref.shape[1]] = rms_rows(
        key_latent_ref[...], latent_gain_ref[...]
    ).astype(jnp.bfloat16)
    repeats = jnp.where(
        lax.broadcasted_iota(jnp.int32, (ROTARY, 128), 0)
        == lax.broadcasted_iota(jnp.int32, (ROTARY, 128), 1) % ROTARY,
        1.0,
        0.0,
    ).astype(jnp.bfloat16)
    own_span = pl.ds(pl.multiple_of(head_index * own_rows, own_rows), own_rows)
    latents[row, core, 0, :, key_latent_ref.shape[1] :] = turn(
        jnp.dot(rotary_key_ref[...], repeats, preferred_element_type=jnp.float32),
        cosine_ref[own_span, :],
        sine_ref[own_span, :],
    )
    queries[row, core] = rms_rows(query_latent_ref[...], query_gain_ref[...]).astype(jnp.bfloat16)
    greet(ep_count, me, head_index)

    def latent_ep(step):
        return remote(
            latents.at[row, core, 0],
            latents.at[row, core, step],
            ep_send.at[1, step],
            ep_recv.at[1, step],
            (lax.rem(me + step, ep_count), head_index),
        )

    def slots_ep(step):
        peer = lax.rem(me + step, ep_count)
        return remote(
            slots_ref.at[peer],
            rows.at[row, core, step],
            ep_send.at[0, step],
            ep_recv.at[0, step],
            (peer, head_index),
        )

    routes_of = {
        "y": (row, y_send, y_recv, y_peer),
        "core": (row, core_send, core_recv, core_peer),
        "cross": (1 - row, cross_send, cross_recv, core_peer),
    }

    def moved(buffer, place, step, route):
        origin_row, send_sem, recv_sem, device = routes_of[route]
        block = buffer.at[origin_row, core] if step == ep_count else buffer.at[origin_row, core, step]
        return remote(block, block, send_sem.at[place, step], recv_sem.at[place, step], device)

    for step in range(1, ep_count):
        latent_ep(step).start()
    for route in ("y", "core"):
        moved(queries, 1, ep_count, route).start()
        moved(latents, 1, 0, route).start()
    expert_normed = rms_rows(expert_input_ref[...], norm_gain_ref[...]).astype(jnp.bfloat16)
    tokens[row, core] = expert_normed
    for route in ("y", "core"):
        moved(tokens, 0, ep_count, route).start()
    expert_total = local_experts * ep_count
    expert_lane = lax.broadcasted_iota(jnp.int32, (own_rows, expert_total), 1)
    named = [
        jnp.where(routes_ref[:, pick : pick + 1] == expert_lane, 1.0, 0.0)
        for pick in range(routes_ref.shape[1])
    ]
    earlier = jnp.where(
        lax.broadcasted_iota(jnp.int32, (own_rows, own_rows), 0)
        > lax.broadcasted_iota(jnp.int32, (own_rows, own_rows), 1),
        1.0,
        0.0,
    ).astype(jnp.bfloat16)
    ahead = jnp.dot(earlier, sum(named).astype(jnp.bfloat16), preferred_element_type=jnp.float32)
    slot_lane = lax.broadcasted_iota(jnp.int32, (own_rows, ep_count * slot_rows), 1)
    picker = jnp.zeros(slot_lane.shape, jnp.float32)
    weight = jnp.zeros(slot_lane.shape, jnp.float32)
    for pick, marks in enumerate(named):
        rank = jnp.sum(ahead * marks, 1, keepdims=True).astype(jnp.int32)
        chosen = slot_lane == routes_ref[:, pick : pick + 1] * capacity + rank
        picker = jnp.where(chosen, 1.0, picker)
        weight = jnp.where(chosen, route_weight_ref[:, pick : pick + 1], weight)
    high = weight.astype(jnp.bfloat16)
    rest = weight - high.astype(jnp.float32)
    middle = rest.astype(jnp.bfloat16)
    weight_ref[:own_rows] = high
    weight_ref[own_rows : 2 * own_rows] = middle
    weight_ref[2 * own_rows :] = (rest - middle.astype(jnp.float32)).astype(jnp.bfloat16)
    picker = picker.T.astype(jnp.bfloat16)
    for start in range(0, width, stripe):
        slots_ref[:, :, start : start + stripe] = (
            jnp.dot(
                picker, expert_normed[:, start : start + stripe], preferred_element_type=jnp.float32
            )
            .astype(jnp.bfloat16)
            .reshape(ep_count, slot_rows, stripe)
        )
    for step in range(1, ep_count):
        slots_ep(step).start()
    own_slots = pltpu.make_async_copy(slots_ref.at[me], rows.at[row, core, 0], own_sem.at[0])
    own_slots.start()
    own_slots.wait()
    for route in ("y", "core"):
        moved(rows, 0, 0, route).start()
    for step in range(1, ep_count):
        latent_ep(step).wait_recv()
        for route in ("y", "core"):
            moved(latents, 1, step, route).start()
    moved(queries, 1, ep_count, "y").wait_recv()
    moved(queries, 1, ep_count, "cross").start()
    moved(tokens, 0, ep_count, "y").wait_recv()
    moved(tokens, 0, ep_count, "cross").start()
    for step in range(ep_count):
        moved(latents, 1, step, "y").wait_recv()
        moved(latents, 1, step, "cross").start()
    for route in ("core", "cross"):
        moved(queries, 1, ep_count, route).wait_recv()
        for step in range(ep_count):
            moved(latents, 1, step, route).wait_recv()

    rank_width = latent_columns_ref.shape[0]
    group_rows = attended.shape[0]

    def project():
        for fetch in fetches[:5]:
            fetch.wait()
        query_rows = queries[...].reshape(group_rows, queries.shape[-1])
        projected = jnp.dot(
            query_rows, query_columns_ref[...], preferred_element_type=jnp.float32
        )
        query_wide[:, :head_lanes] = projected[:, :head_lanes].astype(jnp.bfloat16)
        query_wide[:, head_lanes:] = turn(
            projected[:, head_lanes:], cosine_ref[...], sine_ref[...]
        )
        for block in range(4):
            packed = latents[block // 2, block % 2].reshape(ep_count * own_rows, latents.shape[-1])
            expanded = jnp.dot(
                packed[:, :rank_width],
                latent_columns_ref[...],
                preferred_element_type=jnp.float32,
            ).astype(jnp.bfloat16)
            span = slice(block * ep_count * own_rows, (block + 1) * ep_count * own_rows)
            keys[span, :head_lanes] = expanded[:, :head_lanes]
            keys[span, head_lanes:] = packed[:, rank_width:]
            values[span, :] = expanded[:, head_lanes:]

    def attend(block):
        block_rows = group_rows // 4
        span = slice(block * block_rows, (block + 1) * block_rows)
        query_block = query_wide[span, :]
        lane = lax.broadcasted_iota(jnp.int32, query_block.shape, 1)
        lane_head = jnp.where(
            lane < head_lanes,
            lane // CONTENT,
            (lane - head_lanes) // ROTARY - head_index * heads % (128 // ROTARY),
        )
        out_lane = lax.broadcasted_iota(jnp.int32, (block_rows, head_lanes), 1)
        result = jnp.zeros((block_rows, head_lanes), jnp.float32)
        for head in range(heads):
            chosen = jnp.where(lane_head == head, query_block, jnp.zeros_like(query_block))
            scores = lax.dot_general(
                chosen, keys[...], (((1,), (1,)), ((), ())), preferred_element_type=jnp.float32
            ) * ((CONTENT + ROTARY) ** (-0.5))
            weights = jnp.exp(scores - jnp.max(scores, -1, keepdims=True))
            total = jnp.sum(weights, -1, keepdims=True)
            summed = jnp.dot(
                weights.astype(jnp.bfloat16), values[...], preferred_element_type=jnp.float32
            )
            result = jnp.where(out_lane // VALUE == head, summed / total, result)
        attended[span, :] = result.astype(jnp.bfloat16)

    def mix():
        for start in range(0, width, stripe):
            product = jnp.dot(
                attended[...],
                output_weight_ref[:, start : start + stripe],
                preferred_element_type=jnp.float32,
            ).astype(jnp.bfloat16)
            side[:, :, own_rows:, start : start + stripe] = product.reshape(
                2, 2, own_rows, stripe
            )

    def share():
        for fetch in fetches[5:8]:
            fetch.wait()
        for route in ("core", "cross"):
            moved(tokens, 0, ep_count, route).wait_recv()
        hidden = gated_rows(
            tokens[...].reshape(group_rows, width), shared_gate_ref[...], shared_up_ref[...]
        )
        for start in range(0, width, stripe):
            product = jnp.dot(
                hidden,
                shared_down_ref[:, start : start + stripe],
                preferred_element_type=jnp.float32,
            ).astype(jnp.bfloat16)
            side[:, :, :own_rows, start : start + stripe] = product.reshape(
                2, 2, own_rows, stripe
            )

    def side_half(target_row, place):
        return remote(
            side.at[target_row, 1 - core],
            half_side.at[target_row],
            half_send.at[1, place],
            half_recv.at[1, place],
            core_peer,
        )

    near_side, outer_side = side_half(row, 0), side_half(1 - row, 1)
    side_copy = remote(
        side.at[1 - row, core], far_side, far_send.at[ep_count], far_recv.at[ep_count], y_peer
    )

    def side_exchange():
        outer_side.start()
        near_side.start()

    def side_far():
        outer_side.wait_recv()
        side[1 - row, core] = (
            side[1 - row, core].astype(jnp.float32) + half_side[1 - row].astype(jnp.float32)
        ).astype(jnp.bfloat16)

    tasks = [
        project,
        lambda: attend(0),
        lambda: attend(1),
        lambda: attend(2),
        lambda: attend(3),
        mix,
        share,
        side_exchange,
        side_far,
    ]
    for step in range(max(ep_count + 1, len(tasks))):
        if 0 < step < ep_count:
            slots_ep(step).wait_recv()
            for route in ("y", "core"):
                moved(rows, 0, step, route).start()
        if 0 < step <= ep_count:
            moved(rows, 0, step - 1, "y").wait_recv()
            moved(rows, 0, step - 1, "cross").start()
        if step < len(tasks):
            tasks[step]()
    side_copy.start()
    for fetch in fetches[8:]:
        fetch.wait()
    for route in ("core", "cross"):
        for step in range(ep_count):
            moved(rows, 0, step, route).wait_recv()

    def compute(side_core):
        for expert in range(local_experts):
            span = slice(expert * capacity, (expert + 1) * capacity)
            block = rows[:, side_core, :, span, :].reshape(2 * ep_count * capacity, width)
            hidden = gated_rows(block, gate_ref[expert], up_ref[expert])
            for start in range(0, width, stripe):
                product = jnp.dot(
                    hidden,
                    down_ref[expert, :, start : start + stripe],
                    preferred_element_type=jnp.float32,
                ).astype(jnp.bfloat16)
                part[:, side_core, :, span, start : start + stripe] = product.reshape(
                    2, ep_count, capacity, stripe
                )

    def rows_half(target_row, place):
        return remote(
            part.at[target_row, 1 - core],
            half_rows.at[target_row],
            half_send.at[0, place],
            half_recv.at[0, place],
            core_peer,
        )

    compute(1 - core)
    near, outer = rows_half(row, 0), rows_half(1 - row, 1)
    outer.start()
    near.start()
    compute(core)

    def y_copy(step):
        return remote(
            part.at[1 - row, core, step],
            far_rows.at[step],
            far_send.at[step],
            far_recv.at[step],
            y_peer,
        )

    def back_copy(step):
        return remote(
            part.at[row, core, step],
            returned.at[me],
            back_send.at[step],
            back_recv.at[step],
            (lax.rem(me + ep_count - step, ep_count), head_index),
        )

    outer.wait_recv()
    order = list(range(1, ep_count)) + [0]
    for step in order:
        part[1 - row, core, step] = (
            part[1 - row, core, step].astype(jnp.float32)
            + half_rows[1 - row, step].astype(jnp.float32)
        ).astype(jnp.bfloat16)
        y_copy(step).start()
    near.wait_recv()
    near_side.wait_recv()
    side_copy.wait_recv()
    side_total = (
        side[row, core].astype(jnp.float32)
        + half_side[row].astype(jnp.float32)
        + far_side[...].astype(jnp.float32)
    )
    both_out[0] = side_total[own_rows:]
    for step in order:
        y_copy(step).wait_recv()
        total = (
            part[row, core, step].astype(jnp.float32)
            + half_rows[row, step].astype(jnp.float32)
            + far_rows[step].astype(jnp.float32)
        ).astype(jnp.bfloat16)
        if step > 0:
            part[row, core, step] = total
            back_copy(step).start()
        else:
            returned[me] = total
    for step in range(1, ep_count):
        back_copy(step).wait_recv()
    for start in range(0, width, stripe):
        picked = jnp.dot(
            weight_ref[...],
            returned[:, :, start : start + stripe].reshape(ep_count * slot_rows, stripe),
            preferred_element_type=jnp.float32,
        )
        picked = picked[:own_rows] + picked[own_rows : 2 * own_rows] + picked[2 * own_rows :]
        both_out[1, :, start : start + stripe] = (
            picked + side_total[:own_rows, start : start + stripe]
        )

    for step in range(1, ep_count):
        latent_ep(step).wait_send()
        slots_ep(step).wait_send()
        back_copy(step).wait_send()
    for route in ("y", "core", "cross"):
        moved(queries, 1, ep_count, route).wait_send()
        moved(tokens, 0, ep_count, route).wait_send()
        for step in range(ep_count):
            moved(latents, 1, step, route).wait_send()
            moved(rows, 0, step, route).wait_send()
    for copy in (near, outer, near_side, outer_side, side_copy):
        copy.wait_send()
    for step in range(ep_count):
        y_copy(step).wait_send()


def block_call(ep_count, capacity, *operands):
    query_latent, key_latent = operands[:2]
    own_rows, width = operands[5].shape
    head_lanes = operands[15].shape[0]
    slot_rows = operands[16].shape[0] * capacity
    latent_shape = (own_rows, key_latent.shape[1] + 128)
    vmem = pl.BlockSpec(memory_space=pltpu.VMEM)
    anywhere = pl.BlockSpec(memory_space=pl.ANY)

    def held(*shape):
        return pltpu.VMEM(shape, jnp.bfloat16)

    def sems(*shape):
        return pltpu.SemaphoreType.DMA(shape)

    key_rows = 4 * ep_count * own_rows
    return pl.pallas_call(
        lambda *refs: block_kernel(ep_count, capacity, *refs),
        out_shape=jax.ShapeDtypeStruct((2, own_rows, width), jnp.float32),
        in_specs=[vmem] * 11 + [anywhere] * 11,
        out_specs=vmem,
        scratch_shapes=[
            held(ep_count, slot_rows, width),
            held(query_latent.shape[1], head_lanes + 128),
            held(key_latent.shape[1], 2 * head_lanes),
            held(head_lanes, width),
            held(3 * own_rows, ep_count * slot_rows),
            held(2, 2, ep_count, slot_rows, width),
            held(2, 2, ep_count, *latent_shape),
            held(2, 2, own_rows, width),
            held(2, 2, *query_latent.shape),
        ]
        + [held(*operand.shape) for operand in operands[16:]]
        + [
            held(key_rows, head_lanes + 128),
            held(key_rows, head_lanes),
            held(4 * own_rows, head_lanes + 128),
            held(4 * own_rows, head_lanes),
            held(2, 2, ep_count, slot_rows, width),
            held(2, 2, 2 * own_rows, width),
            held(2, ep_count, slot_rows, width),
            held(2, 2 * own_rows, width),
            held(ep_count, slot_rows, width),
            held(2 * own_rows, width),
            held(ep_count, slot_rows, width),
        ]
        + [sems(2, ep_count + 1)] * 8
        + [
            sems(1),
            sems(11),
            sems(2, 2),
            sems(2, 2),
            sems(ep_count + 1),
            sems(ep_count + 1),
            sems(ep_count),
            sems(ep_count),
        ],
        compiler_params=pltpu.CompilerParams(
            collective_id=0, has_side_effects=True, vmem_limit_bytes=VMEM_LIMIT
        ),
        name="block",
    )(*operands)


def shards(
    query_latent,
    key_latent,
    rotary_key,
    query_gain,
    latent_gain,
    query_content,
    query_rotary,
    key_content,
    value_weight,
    output_weight,
    expert_input,
    norm_gain,
    routes,
    route_weight,
    expert_gate,
    expert_up,
    expert_down,
    shared_gate,
    shared_up,
    shared_down,
):
    group_size = lax.axis_size("tp")
    expert_groups = lax.axis_size("ep")
    token_rows = expert_input.shape[0]
    picks = routes.shape[1]
    local_experts = expert_gate.shape[0]
    expert_total = local_experts * expert_groups
    capacity = 2 * token_rows * picks // expert_total
    if group_size != 4 or capacity % 16:
        return shards_plain(
            query_latent,
            key_latent,
            rotary_key,
            query_gain,
            latent_gain,
            query_content,
            query_rotary,
            key_content,
            value_weight,
            output_weight,
            expert_input,
            norm_gain,
            routes,
            route_weight,
            expert_gate,
            expert_up,
            expert_down,
            shared_gate,
            shared_up,
            shared_down,
        )
    group_rows_count = expert_input.shape[0] * group_size
    positions = lax.axis_index("ep") * group_rows_count + jnp.arange(
        group_rows_count, dtype=jnp.int32
    )
    frequency = rope_base ** (-jnp.arange(ROTARY // 2, dtype=jnp.float32) * 2.0 / ROTARY)
    angles = positions.astype(jnp.float32)[:, None] * jnp.tile(
        jnp.repeat(frequency, 2), 128 // ROTARY
    )[None, :]
    both = block_call(
        expert_groups,
        capacity,
        query_latent,
        key_latent,
        rotary_key,
        query_gain[None, :],
        latent_gain[None, :],
        expert_input,
        norm_gain[None, :],
        routes,
        route_weight,
        jnp.cos(angles),
        jnp.sin(angles),
        query_content,
        query_rotary,
        key_content,
        value_weight,
        output_weight,
        expert_gate,
        expert_up,
        expert_down,
        shared_gate,
        shared_up,
        shared_down,
    )
    return (both[0].astype(jnp.bfloat16), both[1].astype(jnp.bfloat16))


def solution(mesh):
    in_specs = (
        P(("ep", "tp"), None),
        P(("ep", "tp"), None),
        P(("ep", "tp"), None),
        P(),
        P(),
        P(),
        P(),
        P(),
        P(),
        P("tp", None),
        P(("ep", "tp"), None),
        P(),
        P(("ep", "tp"), None),
        P(("ep", "tp"), None),
        P("ep", None, "tp"),
        P("ep", None, "tp"),
        P("ep", "tp", None),
        P(None, "tp"),
        P(None, "tp"),
        P("tp", None),
    )
    out_specs = (P(("ep", "tp"), None), P(("ep", "tp"), None))
    return jax.shard_map(shards, mesh=mesh, in_specs=in_specs, out_specs=out_specs, check_vma=False)
```

```python
import math

import jax
import jax.numpy as jnp
from jax import lax
from jax.experimental import pallas as pl
from jax.experimental.pallas import tpu as pltpu
from jax.sharding import PartitionSpec as P

HEADS = 8
CONTENT = 64
ROTARY = 32
VALUE = 64


norm_eps = 1e-06
rope_base = 10000.0


def rms_rows(entries, gain_row):
    widened = entries.astype(jnp.float32)
    return widened * lax.rsqrt(jnp.mean(widened * widened, -1, keepdims=True) + norm_eps) * gain_row


def turn_pairs(entries, positions):
    width_full = entries.shape[-1]
    frequency = rope_base ** (-jnp.arange(width_full // 2, dtype=jnp.float32) * 2.0 / width_full)
    angles = positions.astype(jnp.float32)[:, None] * frequency[None, :]
    cosine = jnp.cos(angles)[:, None, :]
    sine_part = jnp.sin(angles)[:, None, :]
    even_part = entries[..., 0::2]
    odd_part = entries[..., 1::2]
    joined = jnp.stack(
        [even_part * cosine - odd_part * sine_part, even_part * sine_part + odd_part * cosine], -1
    )
    return joined.reshape(entries.shape)


def absorb_block(carried, query_part, query_turn, key_part, key_turn, value_rows, score_scale):
    running_peak, running_total, summed = carried
    scores = jnp.einsum("qhc,khc->qhk", query_part, key_part, preferred_element_type=jnp.float32)
    scores = scores + jnp.einsum(
        "qhr,kr->qhk", query_turn, key_turn, preferred_element_type=jnp.float32
    )
    scores = scores * score_scale
    new_peak = jnp.maximum(running_peak, jnp.max(scores, -1))
    factor = jnp.exp(running_peak - new_peak)
    weights = jnp.exp(scores - new_peak[..., None])
    running_total = running_total * factor + jnp.sum(weights, -1)
    summed = summed * factor[..., None] + jnp.einsum(
        "qhk,khv->qhv", weights.astype(jnp.bfloat16), value_rows, preferred_element_type=jnp.float32
    )
    return (new_peak, running_total, summed)


def absorb_piece(carried, query_part, query_turn, key_part, key_turn, value_rows, score_scale):
    row_count = key_part.shape[0]
    key_block = math.gcd(row_count, 2048)
    if key_block == row_count:
        return absorb_block(
            carried, query_part, query_turn, key_part, key_turn, value_rows, score_scale
        )
    block_count = row_count // key_block

    def advance(state, pieces):
        return (
            absorb_block(
                state, query_part, query_turn, pieces[0], pieces[1], pieces[2], score_scale
            ),
            None,
        )

    stacked = (
        key_part.reshape((block_count, key_block) + key_part.shape[1:]),
        key_turn.reshape(block_count, key_block, key_turn.shape[1]),
        value_rows.reshape((block_count, key_block) + value_rows.shape[1:]),
    )
    carried, ignored = lax.scan(advance, carried, stacked)
    return carried


def expand_keys(latent_rows, key_columns, value_columns, head_local):
    row_count = latent_rows.shape[0]
    key_part = (
        jnp.dot(latent_rows, key_columns, preferred_element_type=jnp.float32)
        .astype(jnp.bfloat16)
        .reshape(row_count, head_local, CONTENT)
    )
    value_rows = (
        jnp.dot(latent_rows, value_columns, preferred_element_type=jnp.float32)
        .astype(jnp.bfloat16)
        .reshape(row_count, head_local, VALUE)
    )
    return (key_part, value_rows)


def expert_terms(row_block, gate_weight, up_weight, down_weight):
    gated = jnp.einsum("secd,edf->secf", row_block, gate_weight, preferred_element_type=jnp.float32)
    lifted = jnp.einsum("secd,edf->secf", row_block, up_weight, preferred_element_type=jnp.float32)
    hidden = (jax.nn.silu(gated) * lifted).astype(jnp.bfloat16)
    return jnp.einsum("secf,efd->secd", hidden, down_weight, preferred_element_type=jnp.float32)


def shared_terms(row_block, gate_weight, up_weight, down_weight):
    gated = jnp.dot(row_block, gate_weight, preferred_element_type=jnp.float32)
    lifted = jnp.dot(row_block, up_weight, preferred_element_type=jnp.float32)
    hidden = (jax.nn.silu(gated) * lifted).astype(jnp.bfloat16)
    return jnp.dot(hidden, down_weight, preferred_element_type=jnp.float32)


def shards_plain(
    query_latent,
    key_latent,
    rotary_key,
    query_gain,
    latent_gain,
    query_content,
    query_rotary,
    key_content,
    value_weight,
    output_weight,
    expert_input,
    norm_gain,
    routes,
    route_weight,
    expert_gate,
    expert_up,
    expert_down,
    shared_gate,
    shared_up,
    shared_down,
):
    group_size = lax.axis_size("tp")
    expert_groups = lax.axis_size("ep")
    own_rows = query_latent.shape[0]
    head_local = HEADS // group_size
    head_index = lax.axis_index("tp")
    group_rows_count = own_rows * group_size
    group_start = lax.axis_index("ep") * group_rows_count
    own_start = group_start + head_index * own_rows
    score_scale = (CONTENT + ROTARY) ** (-0.5)
    query_normed = rms_rows(query_latent, query_gain).astype(jnp.bfloat16)
    latent_normed = rms_rows(key_latent, latent_gain).astype(jnp.bfloat16)
    own_positions = own_start + jnp.arange(own_rows, dtype=jnp.int32)
    key_turned = turn_pairs(rotary_key.astype(jnp.float32)[:, None, :], own_positions)[
        :, 0, :
    ].astype(jnp.bfloat16)
    token_rows = expert_input.shape[0]
    picks = routes.shape[1]
    local_experts = expert_gate.shape[0]
    expert_total = local_experts * expert_groups
    capacity = 2 * token_rows * picks // expert_total
    slot_total = expert_total * capacity
    model_width = expert_input.shape[1]
    expert_normed = rms_rows(expert_input, norm_gain).astype(jnp.bfloat16)
    flat_routes = routes.reshape(-1)
    marks = (flat_routes[:, None] == jnp.arange(expert_total, dtype=jnp.int32)[None, :]).astype(
        jnp.int32
    )
    ranks = jnp.sum((jnp.cumsum(marks, 0) - marks) * marks, 1)
    targets = flat_routes * capacity + ranks
    picker = (jnp.arange(slot_total, dtype=jnp.int32)[:, None] == targets[None, :]).astype(
        jnp.int32
    )
    picker = jnp.sum(picker.reshape(slot_total, token_rows, picks), 2).astype(jnp.bfloat16)
    outgoing = jnp.dot(picker, expert_normed, preferred_element_type=jnp.float32).astype(
        jnp.bfloat16
    )
    outgoing = outgoing.reshape(expert_groups, local_experts, capacity, model_width)
    received = lax.all_to_all(outgoing, "ep", split_axis=0, concat_axis=0, tiled=True)
    group_query, group_latent, group_turn, gathered_rows, gathered_tokens = (
        lax.all_gather(query_normed, "tp", axis=0, tiled=True),
        lax.all_gather(latent_normed, "tp", axis=0, tiled=True),
        lax.all_gather(key_turned, "tp", axis=0, tiled=True),
        lax.all_gather(received, "tp", axis=0, tiled=True),
        lax.all_gather(expert_normed, "tp", axis=0, tiled=True),
    )
    positions = group_start + jnp.arange(group_rows_count, dtype=jnp.int32)
    content_columns = lax.dynamic_slice_in_dim(
        query_content, head_index * head_local * CONTENT, head_local * CONTENT, 1
    )
    rotary_columns = lax.dynamic_slice_in_dim(
        query_rotary, head_index * head_local * ROTARY, head_local * ROTARY, 1
    )
    query_part = (
        jnp.dot(group_query, content_columns, preferred_element_type=jnp.float32)
        .astype(jnp.bfloat16)
        .reshape(group_rows_count, head_local, CONTENT)
    )
    query_turn = turn_pairs(
        jnp.dot(group_query, rotary_columns, preferred_element_type=jnp.float32).reshape(
            group_rows_count, head_local, ROTARY
        ),
        positions,
    ).astype(jnp.bfloat16)
    key_columns = lax.dynamic_slice_in_dim(
        key_content, head_index * head_local * CONTENT, head_local * CONTENT, 1
    )
    value_columns = lax.dynamic_slice_in_dim(
        value_weight, head_index * head_local * VALUE, head_local * VALUE, 1
    )
    carry_start = (
        jnp.full((group_rows_count, head_local), -jnp.inf, jnp.float32),
        jnp.zeros((group_rows_count, head_local), jnp.float32),
        jnp.zeros((group_rows_count, head_local, VALUE), jnp.float32),
    )
    key_part, value_rows = expand_keys(
        lax.all_gather(group_latent, "ep", axis=0, tiled=True),
        key_columns,
        value_columns,
        head_local,
    )
    running_peak, running_total, summed = absorb_piece(
        carry_start,
        query_part,
        query_turn,
        key_part,
        lax.all_gather(group_turn, "ep", axis=0, tiled=True),
        value_rows,
        score_scale,
    )
    attended = (
        (summed / running_total[..., None])
        .astype(jnp.bfloat16)
        .reshape(group_rows_count, head_local * VALUE)
    )
    routed_term = expert_terms(gathered_rows, expert_gate, expert_up, expert_down)
    shared_term = shared_terms(gathered_tokens, shared_gate, shared_up, shared_down)
    mixer_term = jnp.dot(attended, output_weight, preferred_element_type=jnp.float32)
    mixer_sum, routed_sum, shared_sum = (
        lax.psum_scatter(
            mixer_term.astype(jnp.bfloat16), "tp", scatter_dimension=0, tiled=True
        ).astype(jnp.float32),
        lax.psum_scatter(
            routed_term.astype(jnp.bfloat16), "tp", scatter_dimension=0, tiled=True
        ).astype(jnp.float32),
        lax.psum_scatter(
            shared_term.astype(jnp.bfloat16), "tp", scatter_dimension=0, tiled=True
        ).astype(jnp.float32),
    )
    mixer_out = mixer_sum.astype(jnp.bfloat16)
    returned = lax.all_to_all(
        routed_sum.astype(jnp.bfloat16), "ep", split_axis=0, concat_axis=0, tiled=True
    )
    returned = returned.reshape(slot_total, model_width)
    picked = jnp.take(returned, targets, axis=0).reshape(token_rows, picks, model_width)
    combined = jnp.sum(route_weight[..., None] * picked.astype(jnp.float32), 1) + shared_sum
    expert_out = combined.astype(jnp.bfloat16)
    return (mixer_out, expert_out)


MESH = pl.DeviceIdType.MESH
VMEM_LIMIT = 60 * 1024 * 1024


def greet(ep_count, me, head_index):
    barrier = pltpu.get_barrier_semaphore()
    for step in range(1, ep_count):
        pl.semaphore_signal(
            barrier, inc=1, device_id=(lax.rem(me + step, ep_count), head_index), device_id_type=MESH
        )
    row, core = head_index // 2, head_index % 2
    for other in ((1 - row) * 2 + core, row * 2 + 1 - core):
        pl.semaphore_signal(barrier, inc=1, device_id=(me, other), device_id_type=MESH)
    pl.semaphore_wait(barrier, ep_count + 1)


def gated_rows(rows, gate_weight, up_weight):
    gated = jnp.dot(rows, gate_weight, preferred_element_type=jnp.float32)
    lifted = jnp.dot(rows, up_weight, preferred_element_type=jnp.float32)
    return (gated / (1.0 + jnp.exp(-gated)) * lifted).astype(jnp.bfloat16)


def block_kernel(
    ep_count,
    capacity,
    query_latent_ref,
    key_latent_ref,
    rotary_key_ref,
    query_gain_ref,
    latent_gain_ref,
    expert_input_ref,
    norm_gain_ref,
    routes_ref,
    route_weight_ref,
    cosine_ref,
    sine_ref,
    query_content_hbm,
    query_rotary_hbm,
    key_content_hbm,
    value_weight_hbm,
    output_weight_hbm,
    gate_hbm,
    up_hbm,
    down_hbm,
    shared_gate_hbm,
    shared_up_hbm,
    shared_down_hbm,
    both_out,
    slots_ref,
    query_columns_ref,
    latent_columns_ref,
    output_weight_ref,
    weight_ref,
    rows,
    latents,
    tokens,
    queries,
    gate_ref,
    up_ref,
    down_ref,
    shared_gate_ref,
    shared_up_ref,
    shared_down_ref,
    keys,
    values,
    query_wide,
    attended,
    part,
    side,
    half_rows,
    half_side,
    far_rows,
    far_side,
    returned,
    ep_send,
    ep_recv,
    y_send,
    y_recv,
    core_send,
    core_recv,
    cross_send,
    cross_recv,
    own_sem,
    weight_sem,
    half_send,
    half_recv,
    far_send,
    far_recv,
    back_send,
    back_recv,
):
    me = lax.axis_index("ep")
    head_index = lax.axis_index("tp")
    row, core = head_index // 2, head_index % 2
    y_peer = (me, (1 - row) * 2 + core)
    core_peer = (me, row * 2 + 1 - core)
    local_experts = gate_ref.shape[0]
    width = rows.shape[-1]
    own_rows = tokens.shape[2]
    slot_rows = rows.shape[3]
    stripe = math.gcd(width, 512)

    def remote(source, target, send_sem, recv_sem, device):
        return pltpu.make_async_remote_copy(
            src_ref=source,
            dst_ref=target,
            send_sem=send_sem,
            recv_sem=recv_sem,
            device_id=device,
            device_id_type=MESH,
        )

    head_lanes = attended.shape[1]
    heads = head_lanes // VALUE
    columns = pl.ds(pl.multiple_of(head_index * head_lanes, head_lanes), head_lanes)
    turn_columns = pl.ds(pl.multiple_of(head_index * heads * ROTARY // 128 * 128, 128), 128)
    fetches = [
        pltpu.make_async_copy(source, target, weight_sem.at[place])
        for place, (source, target) in enumerate(
            (
                (query_content_hbm.at[:, columns], query_columns_ref.at[:, :head_lanes]),
                (query_rotary_hbm.at[:, turn_columns], query_columns_ref.at[:, head_lanes:]),
                (key_content_hbm.at[:, columns], latent_columns_ref.at[:, :head_lanes]),
                (value_weight_hbm.at[:, columns], latent_columns_ref.at[:, head_lanes:]),
                (output_weight_hbm, output_weight_ref),
                (shared_gate_hbm, shared_gate_ref),
                (shared_up_hbm, shared_up_ref),
                (shared_down_hbm, shared_down_ref),
                (gate_hbm, gate_ref),
                (up_hbm, up_ref),
                (down_hbm, down_ref),
            )
        )
    ]
    for fetch in fetches:
        fetch.start()

    def turn(entries, cosine, sine):
        lane = lax.broadcasted_iota(jnp.int32, entries.shape, 1)
        crossed = jnp.where(
            lane % 2 == 0, -pltpu.roll(entries, 127, 1), pltpu.roll(entries, 1, 1)
        )
        return (entries * cosine + crossed * sine).astype(jnp.bfloat16)

    latents[row, core, 0, :, : key_latent_ref.shape[1]] = rms_rows(
        key_latent_ref[...], latent_gain_ref[...]
    ).astype(jnp.bfloat16)
    repeats = jnp.where(
        lax.broadcasted_iota(jnp.int32, (ROTARY, 128), 0)
        == lax.broadcasted_iota(jnp.int32, (ROTARY, 128), 1) % ROTARY,
        1.0,
        0.0,
    ).astype(jnp.bfloat16)
    own_span = pl.ds(pl.multiple_of(head_index * own_rows, own_rows), own_rows)
    latents[row, core, 0, :, key_latent_ref.shape[1] :] = turn(
        lax.dot_general(
            rotary_key_ref[...],
            repeats,
            (((0,), (0,)), ((), ())),
            preferred_element_type=jnp.float32,
        ),
        cosine_ref[own_span, :],
        sine_ref[own_span, :],
    )
    queries[row, core] = rms_rows(query_latent_ref[...], query_gain_ref[...]).astype(jnp.bfloat16)
    greet(ep_count, me, head_index)

    def latent_ep(step):
        return remote(
            latents.at[row, core, 0],
            latents.at[row, core, step],
            ep_send.at[1, step],
            ep_recv.at[1, step],
            (lax.rem(me + step, ep_count), head_index),
        )

    def slots_ep(step):
        peer = lax.rem(me + step, ep_count)
        return remote(
            slots_ref.at[peer],
            rows.at[row, core, step],
            ep_send.at[0, step],
            ep_recv.at[0, step],
            (peer, head_index),
        )

    routes_of = {
        "y": (row, y_send, y_recv, y_peer),
        "core": (row, core_send, core_recv, core_peer),
        "cross": (1 - row, cross_send, cross_recv, core_peer),
    }

    def moved(buffer, place, step, route):
        origin_row, send_sem, recv_sem, device = routes_of[route]
        block = buffer.at[origin_row, core] if step == ep_count else buffer.at[origin_row, core, step]
        return remote(block, block, send_sem.at[place, step], recv_sem.at[place, step], device)

    for step in range(1, ep_count):
        latent_ep(step).start()
    for route in ("y", "core"):
        moved(queries, 1, ep_count, route).start()
        moved(latents, 1, 0, route).start()
    expert_normed = rms_rows(expert_input_ref[...], norm_gain_ref[...]).astype(jnp.bfloat16)
    tokens[row, core] = expert_normed
    for route in ("y", "core"):
        moved(tokens, 0, ep_count, route).start()
    expert_total = local_experts * ep_count
    expert_lane = lax.broadcasted_iota(jnp.int32, (own_rows, expert_total), 1)
    route_columns = routes_ref[...].T
    weight_columns = route_weight_ref[...].T
    named = [
        jnp.where(route_columns[:, pick : pick + 1] == expert_lane, 1.0, 0.0)
        for pick in range(routes_ref.shape[0])
    ]
    earlier = jnp.where(
        lax.broadcasted_iota(jnp.int32, (own_rows, own_rows), 0)
        > lax.broadcasted_iota(jnp.int32, (own_rows, own_rows), 1),
        1.0,
        0.0,
    ).astype(jnp.bfloat16)
    ahead = jnp.dot(earlier, sum(named).astype(jnp.bfloat16), preferred_element_type=jnp.float32)
    slot_lane = lax.broadcasted_iota(jnp.int32, (own_rows, ep_count * slot_rows), 1)
    picker = jnp.zeros(slot_lane.shape, jnp.float32)
    weight = jnp.zeros(slot_lane.shape, jnp.float32)
    for pick, marks in enumerate(named):
        rank = jnp.sum(ahead * marks, 1, keepdims=True).astype(jnp.int32)
        chosen = slot_lane == route_columns[:, pick : pick + 1] * capacity + rank
        picker = jnp.where(chosen, 1.0, picker)
        weight = jnp.where(chosen, weight_columns[:, pick : pick + 1], weight)
    high = weight.astype(jnp.bfloat16)
    rest = weight - high.astype(jnp.float32)
    middle = rest.astype(jnp.bfloat16)
    weight_ref[:own_rows] = high
    weight_ref[own_rows : 2 * own_rows] = middle
    weight_ref[2 * own_rows :] = (rest - middle.astype(jnp.float32)).astype(jnp.bfloat16)
    picker = picker.T.astype(jnp.bfloat16)
    for start in range(0, width, stripe):
        slots_ref[:, :, start : start + stripe] = (
            jnp.dot(
                picker, expert_normed[:, start : start + stripe], preferred_element_type=jnp.float32
            )
            .astype(jnp.bfloat16)
            .reshape(ep_count, slot_rows, stripe)
        )
    for step in range(1, ep_count):
        slots_ep(step).start()
    own_slots = pltpu.make_async_copy(slots_ref.at[me], rows.at[row, core, 0], own_sem.at[0])
    own_slots.start()
    own_slots.wait()
    for route in ("y", "core"):
        moved(rows, 0, 0, route).start()
    for step in range(1, ep_count):
        latent_ep(step).wait_recv()
        for route in ("y", "core"):
            moved(latents, 1, step, route).start()
    moved(queries, 1, ep_count, "y").wait_recv()
    moved(queries, 1, ep_count, "cross").start()
    moved(tokens, 0, ep_count, "y").wait_recv()
    moved(tokens, 0, ep_count, "cross").start()
    for step in range(ep_count):
        moved(latents, 1, step, "y").wait_recv()
        moved(latents, 1, step, "cross").start()
    for route in ("core", "cross"):
        moved(queries, 1, ep_count, route).wait_recv()
        for step in range(ep_count):
            moved(latents, 1, step, route).wait_recv()

    rank_width = latent_columns_ref.shape[0]
    group_rows = attended.shape[0]

    def project():
        for fetch in fetches[:5]:
            fetch.wait()
        query_rows = queries[...].reshape(group_rows, queries.shape[-1])
        projected = jnp.dot(
            query_rows, query_columns_ref[...], preferred_element_type=jnp.float32
        )
        query_wide[:, :head_lanes] = projected[:, :head_lanes].astype(jnp.bfloat16)
        query_wide[:, head_lanes:] = turn(
            projected[:, head_lanes:], cosine_ref[...], sine_ref[...]
        )
        for block in range(4):
            packed = latents[block // 2, block % 2].reshape(ep_count * own_rows, latents.shape[-1])
            expanded = jnp.dot(
                packed[:, :rank_width],
                latent_columns_ref[...],
                preferred_element_type=jnp.float32,
            ).astype(jnp.bfloat16)
            span = slice(block * ep_count * own_rows, (block + 1) * ep_count * own_rows)
            keys[span, :head_lanes] = expanded[:, :head_lanes]
            keys[span, head_lanes:] = packed[:, rank_width:]
            values[span, :] = expanded[:, head_lanes:]

    def attend(block):
        block_rows = group_rows // 4
        span = slice(block * block_rows, (block + 1) * block_rows)
        query_block = query_wide[span, :]
        lane = lax.broadcasted_iota(jnp.int32, query_block.shape, 1)
        lane_head = jnp.where(
            lane < head_lanes,
            lane // CONTENT,
            (lane - head_lanes) // ROTARY - head_index * heads % (128 // ROTARY),
        )
        out_lane = lax.broadcasted_iota(jnp.int32, (block_rows, head_lanes), 1)
        result = jnp.zeros((block_rows, head_lanes), jnp.float32)
        for head in range(heads):
            chosen = jnp.where(lane_head == head, query_block, jnp.zeros_like(query_block))
            scores = lax.dot_general(
                chosen, keys[...], (((1,), (1,)), ((), ())), preferred_element_type=jnp.float32
            ) * ((CONTENT + ROTARY) ** (-0.5))
            weights = jnp.exp(scores - jnp.max(scores, -1, keepdims=True))
            total = jnp.sum(weights, -1, keepdims=True)
            summed = jnp.dot(
                weights.astype(jnp.bfloat16), values[...], preferred_element_type=jnp.float32
            )
            result = jnp.where(out_lane // VALUE == head, summed / total, result)
        attended[span, :] = result.astype(jnp.bfloat16)

    def mix():
        for start in range(0, width, stripe):
            product = jnp.dot(
                attended[...],
                output_weight_ref[:, start : start + stripe],
                preferred_element_type=jnp.float32,
            ).astype(jnp.bfloat16)
            side[:, :, own_rows:, start : start + stripe] = product.reshape(
                2, 2, own_rows, stripe
            )

    def share():
        for fetch in fetches[5:8]:
            fetch.wait()
        for route in ("core", "cross"):
            moved(tokens, 0, ep_count, route).wait_recv()
        hidden = gated_rows(
            tokens[...].reshape(group_rows, width), shared_gate_ref[...], shared_up_ref[...]
        )
        for start in range(0, width, stripe):
            product = jnp.dot(
                hidden,
                shared_down_ref[:, start : start + stripe],
                preferred_element_type=jnp.float32,
            ).astype(jnp.bfloat16)
            side[:, :, :own_rows, start : start + stripe] = product.reshape(
                2, 2, own_rows, stripe
            )

    def side_half(target_row, place):
        return remote(
            side.at[target_row, 1 - core],
            half_side.at[target_row],
            half_send.at[1, place],
            half_recv.at[1, place],
            core_peer,
        )

    near_side, outer_side = side_half(row, 0), side_half(1 - row, 1)
    side_copy = remote(
        side.at[1 - row, core], far_side, far_send.at[ep_count], far_recv.at[ep_count], y_peer
    )

    def side_exchange():
        outer_side.start()
        near_side.start()

    def side_far():
        outer_side.wait_recv()
        side[1 - row, core] = (
            side[1 - row, core].astype(jnp.float32) + half_side[1 - row].astype(jnp.float32)
        ).astype(jnp.bfloat16)

    tasks = [
        project,
        lambda: attend(0),
        lambda: attend(1),
        lambda: attend(2),
        lambda: attend(3),
        mix,
        share,
        side_exchange,
        side_far,
    ]
    for step in range(max(ep_count + 1, len(tasks))):
        if 0 < step < ep_count:
            slots_ep(step).wait_recv()
            for route in ("y", "core"):
                moved(rows, 0, step, route).start()
        if 0 < step <= ep_count:
            moved(rows, 0, step - 1, "y").wait_recv()
            moved(rows, 0, step - 1, "cross").start()
        if step < len(tasks):
            tasks[step]()
    side_copy.start()
    for fetch in fetches[8:]:
        fetch.wait()
    for route in ("core", "cross"):
        for step in range(ep_count):
            moved(rows, 0, step, route).wait_recv()

    def compute(side_core):
        for expert in range(local_experts):
            span = slice(expert * capacity, (expert + 1) * capacity)
            block = rows[:, side_core, :, span, :].reshape(2 * ep_count * capacity, width)
            hidden = gated_rows(block, gate_ref[expert], up_ref[expert])
            for start in range(0, width, stripe):
                product = jnp.dot(
                    hidden,
                    down_ref[expert, :, start : start + stripe],
                    preferred_element_type=jnp.float32,
                ).astype(jnp.bfloat16)
                part[:, side_core, :, span, start : start + stripe] = product.reshape(
                    2, ep_count, capacity, stripe
                )

    def rows_half(target_row, place):
        return remote(
            part.at[target_row, 1 - core],
            half_rows.at[target_row],
            half_send.at[0, place],
            half_recv.at[0, place],
            core_peer,
        )

    compute(1 - core)
    near, outer = rows_half(row, 0), rows_half(1 - row, 1)
    outer.start()
    near.start()
    compute(core)

    def y_copy(step):
        return remote(
            part.at[1 - row, core, step],
            far_rows.at[step],
            far_send.at[step],
            far_recv.at[step],
            y_peer,
        )

    def back_copy(step):
        return remote(
            part.at[row, core, step],
            returned.at[me],
            back_send.at[step],
            back_recv.at[step],
            (lax.rem(me + ep_count - step, ep_count), head_index),
        )

    outer.wait_recv()
    order = list(range(1, ep_count)) + [0]
    for step in order:
        part[1 - row, core, step] = (
            part[1 - row, core, step].astype(jnp.float32)
            + half_rows[1 - row, step].astype(jnp.float32)
        ).astype(jnp.bfloat16)
        y_copy(step).start()
    near.wait_recv()
    near_side.wait_recv()
    side_copy.wait_recv()
    side_total = (
        side[row, core].astype(jnp.float32)
        + half_side[row].astype(jnp.float32)
        + far_side[...].astype(jnp.float32)
    )
    both_out[0] = side_total[own_rows:].astype(jnp.bfloat16)
    for step in order:
        y_copy(step).wait_recv()
        total = (
            part[row, core, step].astype(jnp.float32)
            + half_rows[row, step].astype(jnp.float32)
            + far_rows[step].astype(jnp.float32)
        ).astype(jnp.bfloat16)
        if step > 0:
            part[row, core, step] = total
            back_copy(step).start()
        else:
            returned[me] = total
    for step in range(1, ep_count):
        back_copy(step).wait_recv()
    for start in range(0, width, stripe):
        picked = jnp.dot(
            weight_ref[...],
            returned[:, :, start : start + stripe].reshape(ep_count * slot_rows, stripe),
            preferred_element_type=jnp.float32,
        )
        picked = picked[:own_rows] + picked[own_rows : 2 * own_rows] + picked[2 * own_rows :]
        both_out[1, :, start : start + stripe] = (
            picked + side_total[:own_rows, start : start + stripe]
        ).astype(jnp.bfloat16)

    for step in range(1, ep_count):
        latent_ep(step).wait_send()
        slots_ep(step).wait_send()
        back_copy(step).wait_send()
    for route in ("y", "core", "cross"):
        moved(queries, 1, ep_count, route).wait_send()
        moved(tokens, 0, ep_count, route).wait_send()
        for step in range(ep_count):
            moved(latents, 1, step, route).wait_send()
            moved(rows, 0, step, route).wait_send()
    for copy in (near, outer, near_side, outer_side, side_copy):
        copy.wait_send()
    for step in range(ep_count):
        y_copy(step).wait_send()


def block_call(ep_count, capacity, *operands):
    query_latent, key_latent = operands[:2]
    own_rows, width = operands[5].shape
    head_lanes = operands[15].shape[0]
    slot_rows = operands[16].shape[0] * capacity
    latent_shape = (own_rows, key_latent.shape[1] + 128)
    vmem = pl.BlockSpec(memory_space=pltpu.VMEM)
    anywhere = pl.BlockSpec(memory_space=pl.ANY)

    def held(*shape):
        return pltpu.VMEM(shape, jnp.bfloat16)

    def sems(*shape):
        return pltpu.SemaphoreType.DMA(shape)

    key_rows = 4 * ep_count * own_rows
    return pl.pallas_call(
        lambda *refs: block_kernel(ep_count, capacity, *refs),
        out_shape=jax.ShapeDtypeStruct((2, own_rows, width), jnp.bfloat16),
        in_specs=[vmem] * 11 + [anywhere] * 11,
        out_specs=vmem,
        scratch_shapes=[
            held(ep_count, slot_rows, width),
            held(query_latent.shape[1], head_lanes + 128),
            held(key_latent.shape[1], 2 * head_lanes),
            held(head_lanes, width),
            held(3 * own_rows, ep_count * slot_rows),
            held(2, 2, ep_count, slot_rows, width),
            held(2, 2, ep_count, *latent_shape),
            held(2, 2, own_rows, width),
            held(2, 2, *query_latent.shape),
        ]
        + [held(*operand.shape) for operand in operands[16:]]
        + [
            held(key_rows, head_lanes + 128),
            held(key_rows, head_lanes),
            held(4 * own_rows, head_lanes + 128),
            held(4 * own_rows, head_lanes),
            held(2, 2, ep_count, slot_rows, width),
            held(2, 2, 2 * own_rows, width),
            held(2, ep_count, slot_rows, width),
            held(2, 2 * own_rows, width),
            held(ep_count, slot_rows, width),
            held(2 * own_rows, width),
            held(ep_count, slot_rows, width),
        ]
        + [sems(2, ep_count + 1)] * 8
        + [
            sems(1),
            sems(11),
            sems(2, 2),
            sems(2, 2),
            sems(ep_count + 1),
            sems(ep_count + 1),
            sems(ep_count),
            sems(ep_count),
        ],
        compiler_params=pltpu.CompilerParams(
            collective_id=0, has_side_effects=True, vmem_limit_bytes=VMEM_LIMIT
        ),
        name="block",
    )(*operands)


def shards(
    query_latent,
    key_latent,
    rotary_key,
    query_gain,
    latent_gain,
    query_content,
    query_rotary,
    key_content,
    value_weight,
    output_weight,
    expert_input,
    norm_gain,
    routes,
    route_weight,
    expert_gate,
    expert_up,
    expert_down,
    shared_gate,
    shared_up,
    shared_down,
):
    group_size = lax.axis_size("tp")
    expert_groups = lax.axis_size("ep")
    token_rows = expert_input.shape[0]
    picks = routes.shape[1]
    local_experts = expert_gate.shape[0]
    expert_total = local_experts * expert_groups
    capacity = 2 * token_rows * picks // expert_total
    if group_size != 4 or capacity % 16:
        return shards_plain(
            query_latent,
            key_latent,
            rotary_key,
            query_gain,
            latent_gain,
            query_content,
            query_rotary,
            key_content,
            value_weight,
            output_weight,
            expert_input,
            norm_gain,
            routes,
            route_weight,
            expert_gate,
            expert_up,
            expert_down,
            shared_gate,
            shared_up,
            shared_down,
        )
    group_rows_count = expert_input.shape[0] * group_size
    positions = lax.axis_index("ep") * group_rows_count + jnp.arange(
        group_rows_count, dtype=jnp.int32
    )
    frequency = rope_base ** (-jnp.arange(ROTARY // 2, dtype=jnp.float32) * 2.0 / ROTARY)
    angles = positions.astype(jnp.float32)[:, None] * jnp.tile(
        jnp.repeat(frequency, 2), 128 // ROTARY
    )[None, :]
    both = block_call(
        expert_groups,
        capacity,
        query_latent,
        key_latent,
        rotary_key.T,
        query_gain[None, :],
        latent_gain[None, :],
        expert_input,
        norm_gain[None, :],
        routes.T,
        route_weight.T,
        jnp.cos(angles),
        jnp.sin(angles),
        query_content,
        query_rotary,
        key_content,
        value_weight,
        output_weight,
        expert_gate,
        expert_up,
        expert_down,
        shared_gate,
        shared_up,
        shared_down,
    )
    return (both[0], both[1])


def solution(mesh):
    in_specs = (
        P(("ep", "tp"), None),
        P(("ep", "tp"), None),
        P(("ep", "tp"), None),
        P(),
        P(),
        P(),
        P(),
        P(),
        P(),
        P("tp", None),
        P(("ep", "tp"), None),
        P(),
        P(("ep", "tp"), None),
        P(("ep", "tp"), None),
        P("ep", None, "tp"),
        P("ep", None, "tp"),
        P("ep", "tp", None),
        P(None, "tp"),
        P(None, "tp"),
        P("tp", None),
    )
    out_specs = (P(("ep", "tp"), None), P(("ep", "tp"), None))
    return jax.shard_map(shards, mesh=mesh, in_specs=in_specs, out_specs=out_specs, check_vma=False)
```
